512 devices in a mesh: sp: 64 (over z, y), tp: 8 (over x, core).
Axes of the slice: x: 4, y: 4, z: 16, core: 2. Of those that a mesh axis runs over, the one named last changes fastest.
Arguments:
- tokens: bfloat16 [8192, 2048], P(('sp', 'tp')), may hold values from -6 to 6
- input_norm_gain: float32 [2048], replicated, may hold values from 0.1 to 1.9
- differential_query: bfloat16 [2048, 1024], P(None, 'tp'), may hold values from -0.176776695 to 0.176776695, as said below
- differential_key: bfloat16 [2048, 1024], P(None, 'tp'), may hold values from -0.176776695 to 0.176776695, as said below
- differential_value: bfloat16 [2048, 1024], P(None, 'tp'), may hold values from -0.125 to 0.125
- query_norm_gain: float32 [64], replicated, may hold values from 1.15 to 5
- key_norm_gain: float32 [64], replicated, may hold values from 1.15 to 5
- second_map_weight: float32 [8], P('tp'), may hold values from 0.3 to 0.8
- differential_norm_gain: float32 [128], replicated, may hold values from 0.1 to 1.9
- linear_query: bfloat16 [2048, 512], P(None, 'tp'), may hold values from -0.125 to 0.125
- linear_key: bfloat16 [2048, 512], P(None, 'tp'), may hold values from -0.125 to 0.125
- linear_value: bfloat16 [2048, 1024], P(None, 'tp'), may hold values from -0.125 to 0.125
- linear_output_gate: bfloat16 [2048, 1024], P(None, 'tp'), may hold values from -0.125 to 0.125
- forget_down_factor: bfloat16 [2048, 32], replicated, may hold values from -0.125 to 0.125
- forget_up_factor: bfloat16 [32, 512], P(None, 'tp'), may hold values from -2.109375 to 2.109375
- forget_bias: float32 [512], P('tp'), may hold values from -0.5 to 10
- extra_shrinkage_exponent: float32 [8192, 8], P('sp', 'tp'), may hold values from -1.5 to 0
- linear_norm_gain: float32 [128], replicated, may hold values from 0.1 to 1.9
- differential_output_rows: bfloat16 [1024, 2048], P('tp'), may hold values from -0.125 to 0.125
- linear_output_rows: bfloat16 [1024, 2048], P('tp'), may hold values from -0.125 to 0.125
Outputs:
- layer_out: bfloat16 [8192, 2048], P(('sp', 'tp'))
The draws below stay inside these ranges and needn't reach their ends.
Inputs may be any that keep to these rules, and one draw needn't show every extreme that they name: `differential_query`: independent entries of scale one over sqrt(2048). `differential_key`: entries of scale one over sqrt(2048).
All inputs are finite; a program needn't handle non-finite values.
Results may differ from the reference program's by a relative error of at most 0.015.
Values may be sent and summed in bfloat16 or wider, within the bound.
No kernel may reach another device: no remote copies, remote signals or barrier semaphores. Data moves between devices by JAX's collectives and lax.ppermute only.
A program may use at most 64 MiB of HBM per device.

```python
import math
import jax
import jax.numpy as jnp
from jax import lax

D = 2048
DA_HEADS = 8
HEAD = 64
VDIM = 128
RECURRENT_LANES = 8
RECURRENT_DIM = 64
GLA_DV = 128
RANK = 32
BLOCK = 64
TOK_DEV = 128
SEQUENCE_LENGTH = 8192
N_SP = 64
N_TP = 8


def attn_pair(key):
    base_part = jnp.clip(jax.random.normal(jax.random.fold_in(key, 11), (D, DA_HEADS * 2 * HEAD), jnp.float32), -6.0, 6.0)
    noise_part = jnp.clip(jax.random.normal(jax.random.fold_in(key, 12), (D, DA_HEADS * 2 * HEAD), jnp.float32), -6.0, 6.0)
    key_weight = noise_part
    return (base_part * D ** (-0.5), key_weight * D ** (-0.5))


def draw_differential_query(key, part):
    return attn_pair(key)[0].astype(jnp.bfloat16)


def draw_differential_key(key, part):
    return attn_pair(key)[1].astype(jnp.bfloat16)


def gain_draw(key):
    values = jax.random.uniform(key, (HEAD,), jnp.float32, 1.15, 1.45)
    return values


def draw_query_norm_gain(key, part):
    return gain_draw(jax.random.fold_in(key, 31))


def draw_key_norm_gain(key, part):
    return gain_draw(jax.random.fold_in(key, 32))


def draw_forget_bias(key, part):
    ranking = jax.random.permutation(jax.random.fold_in(key, 41), RECURRENT_LANES)
    fast_heads = ranking < RECURRENT_LANES // 2
    fast_bias = jax.random.uniform(jax.random.fold_in(key, 42), (RECURRENT_LANES, RECURRENT_DIM), jnp.float32, -0.5, 0.5)
    slow_bias = jax.random.uniform(jax.random.fold_in(key, 43), (RECURRENT_LANES, RECURRENT_DIM), jnp.float32, 8.0, 10.0)
    return jnp.where(fast_heads[:, None], fast_bias, slow_bias).reshape(RECURRENT_LANES * RECURRENT_DIM)


def draw_extra_shrinkage_exponent(key, part):
    block_total = SEQUENCE_LENGTH // TOK_DEV
    block_rates = jnp.exp(jax.random.uniform(jax.random.fold_in(key, 51), (block_total, 1, RECURRENT_LANES), jnp.float32, math.log(0.2), math.log(1.0))) / SEQUENCE_LENGTH
    baseline_rate = -jnp.broadcast_to(block_rates, (block_total, TOK_DEV, RECURRENT_LANES)).reshape(SEQUENCE_LENGTH, RECURRENT_LANES)
    spike_positions = jax.random.randint(jax.random.fold_in(key, 52), (3,), 0, SEQUENCE_LENGTH)
    spike_drops = jnp.log(jax.random.uniform(jax.random.fold_in(key, 53), (3, RECURRENT_LANES), jnp.float32, 0.5, 0.8))
    spike_hits = (jnp.arange(SEQUENCE_LENGTH, dtype=jnp.int32)[:, None] == spike_positions[None, :]).astype(jnp.float32)
    return baseline_rate + jnp.dot(spike_hits, spike_drops)


def level_of(rng, dims, pieces, smallest, largest):
    gain = 1.0
    for position, parts in pieces:
        steps = jax.random.uniform(jax.random.fold_in(jax.random.fold_in(rng, 6), position), (parts,), jnp.float32, smallest / len(pieces), largest / len(pieces))
        gain = gain * jnp.repeat(jnp.exp(steps), dims[position] // parts).reshape((-1,) + (1,) * (len(dims) - 1 - position))
    return gain


def centred(key, dims, scale, most, split=(), kind=jnp.bfloat16):
    values = jax.random.normal(key, dims, jnp.float32) * scale
    if len(split) > 0:
        values = level_of(key, dims, split, -0.22, 0.18) * values
    return jnp.clip(values, min=-most, max=most).astype(kind)


def setup_inputs(seed: int = 0) -> dict:
    arg_keys = jax.random.split(jax.random.key(seed), 21)
    tokens = centred(arg_keys[0], (SEQUENCE_LENGTH, D), 1.0, 6.0, ((0, 512),))
    input_norm_gain = jnp.clip(1.0 + 0.18 * jax.random.normal(arg_keys[1], (D,), jnp.float32), 0.1, 1.9)
    differential_query = draw_differential_query(jax.random.fold_in(arg_keys[20], 71), 0)
    differential_key = draw_differential_key(jax.random.fold_in(arg_keys[20], 71), 0)
    differential_value = centred(arg_keys[4], (D, DA_HEADS * VDIM), D ** -0.5, 0.125, ((1, 8),))
    query_norm_gain = draw_query_norm_gain(jax.random.fold_in(arg_keys[20], 71), 0)
    key_norm_gain = draw_key_norm_gain(jax.random.fold_in(arg_keys[20], 71), 0)
    second_map_weight = jnp.clip(0.3 + 0.5 * jax.random.uniform(arg_keys[7], (DA_HEADS,), jnp.float32) ** level_of(arg_keys[7], (DA_HEADS,), ((0, 8),), -0.2, 0.2), 0.3, 0.8)
    differential_norm_gain = jnp.clip(1.0 + 0.18 * jax.random.normal(arg_keys[8], (VDIM,), jnp.float32), 0.1, 1.9)
    linear_query = centred(arg_keys[9], (D, RECURRENT_LANES * RECURRENT_DIM), D ** -0.5, 0.125, ((1, 8),))
    linear_key = centred(arg_keys[10], (D, RECURRENT_LANES * RECURRENT_DIM), D ** -0.5, 0.125, ((1, 8),))
    linear_value = centred(arg_keys[11], (D, RECURRENT_LANES * GLA_DV), D ** -0.5, 0.125, ((1, 8),))
    linear_output_gate = centred(arg_keys[12], (D, RECURRENT_LANES * GLA_DV), D ** -0.5, 0.125, ((1, 8),))
    forget_down_factor = centred(arg_keys[13], (D, RANK), D ** -0.5, 0.125)
    forget_up_factor = centred(arg_keys[14], (RANK, RECURRENT_LANES * RECURRENT_DIM), (2.0 * RANK ** -0.5), 2.109375, ((1, 8),))
    forget_bias = draw_forget_bias(jax.random.fold_in(arg_keys[20], 71), 0)
    extra_shrinkage_exponent = draw_extra_shrinkage_exponent(jax.random.fold_in(arg_keys[20], 71), 0)
    linear_norm_gain = jnp.clip(1.0 + 0.18 * jax.random.normal(arg_keys[17], (GLA_DV,), jnp.float32), 0.1, 1.9)
    differential_output_rows = centred(arg_keys[18], (DA_HEADS * VDIM, D), (DA_HEADS * VDIM + RECURRENT_LANES * GLA_DV) ** -0.5, 0.125, ((0, 8),))
    linear_output_rows = centred(arg_keys[19], (RECURRENT_LANES * GLA_DV, D), (DA_HEADS * VDIM + RECURRENT_LANES * GLA_DV) ** -0.5, 0.125, ((0, 8),))
    return dict(tokens=tokens, input_norm_gain=input_norm_gain, differential_query=differential_query, differential_key=differential_key, differential_value=differential_value, query_norm_gain=query_norm_gain, key_norm_gain=key_norm_gain, second_map_weight=second_map_weight, differential_norm_gain=differential_norm_gain, linear_query=linear_query, linear_key=linear_key, linear_value=linear_value, linear_output_gate=linear_output_gate, forget_down_factor=forget_down_factor, forget_up_factor=forget_up_factor, forget_bias=forget_bias, extra_shrinkage_exponent=extra_shrinkage_exponent, linear_norm_gain=linear_norm_gain, differential_output_rows=differential_output_rows, linear_output_rows=linear_output_rows)


RMS_EPS = 1e-06
SOFTMAX_DIVISOR = 16.0
OUT_SCALE = 0.8
HIGHEST = lax.Precision.HIGHEST

def rms_scale(values, scale_gain):
    mean_sq = lax.optimization_barrier(jnp.mean(values * values, axis=-1, keepdims=True))
    return values * lax.rsqrt(mean_sq + RMS_EPS) * scale_gain

def attention_reference(query_norm, key_norm, value_rows, second_map_weight):
    positions = jnp.arange(SEQUENCE_LENGTH, dtype=jnp.int32)

    def one_head(inputs):
        query_head, key_head, value_head, lambda_value = inputs
        key_float = key_head.astype(jnp.float32)

        def one_block(first_row):
            query_block = lax.dynamic_slice_in_dim(query_head, first_row, TOK_DEV, 0).astype(jnp.float32)
            scores = jnp.einsum('tmd,kmd->mtk', query_block, key_float) * HEAD ** (-0.5)
            query_pos = first_row + jnp.arange(TOK_DEV, dtype=jnp.int32)
            causal = positions[None, :] <= query_pos[:, None]
            scores = jnp.where(causal[None], scores, -jnp.inf)
            row_peak = lax.optimization_barrier(jnp.max(scores, axis=-1, keepdims=True))
            weights = jnp.exp(scores - row_peak)
            totals = lax.optimization_barrier(jnp.sum(weights, axis=-1))
            first_map = jnp.dot(weights[0].astype(jnp.bfloat16), value_head, preferred_element_type=jnp.float32) / totals[0][:, None]
            second = jnp.dot(weights[1].astype(jnp.bfloat16), value_head, preferred_element_type=jnp.float32) / totals[1][:, None]
            return first_map - lambda_value * second
        starts = jnp.arange(N_SP, dtype=jnp.int32) * TOK_DEV
        return lax.map(one_block, starts).reshape(SEQUENCE_LENGTH, VDIM)
    return lax.map(one_head, (query_norm.transpose(1, 0, 2, 3), key_norm.transpose(1, 0, 2, 3), value_rows.transpose(1, 0, 2), second_map_weight))

def chain_reference(queries, keys_rows, values_rows, shrinkage_exponent):
    blocks = SEQUENCE_LENGTH // BLOCK

    def blockify(array):
        return array.reshape(blocks, BLOCK, RECURRENT_LANES, array.shape[-1])
    causal = jnp.tril(jnp.ones((BLOCK, BLOCK), dtype=bool))

    def step_block(carried, inputs):
        query_block, key_block, value_block, decay_block = inputs
        log_cum = jnp.cumsum(decay_block, axis=0)
        inter = jnp.einsum('thd,hde->the', query_block * jnp.exp(log_cum), carried, precision=HIGHEST)
        differences = log_cum[:, None] - log_cum[None, :]
        decay_table = jnp.exp(jnp.where(causal[:, :, None, None], differences, -jnp.inf))
        inner_scores = jnp.einsum('thd,shd,tshd->hts', query_block, key_block, decay_table, precision=HIGHEST)
        intra = jnp.einsum('hts,she->the', inner_scores, value_block, precision=HIGHEST)
        log_last = log_cum[-1]
        key_end = key_block * jnp.exp(log_last[None] - log_cum)
        carried = carried * jnp.exp(log_last)[..., None] + jnp.einsum('thd,the->hde', key_end, value_block, precision=HIGHEST)
        return (carried, inter + intra)
    state_zero = jnp.zeros((RECURRENT_LANES, RECURRENT_DIM, GLA_DV), jnp.float32)
    _, outputs = lax.scan(step_block, state_zero, (blockify(queries), blockify(keys_rows), blockify(values_rows), blockify(shrinkage_exponent)))
    return outputs.reshape(SEQUENCE_LENGTH, RECURRENT_LANES, GLA_DV)

def reference(tokens, input_norm_gain, differential_query, differential_key, differential_value, query_norm_gain, key_norm_gain, second_map_weight, differential_norm_gain, linear_query, linear_key, linear_value, linear_output_gate, forget_down_factor, forget_up_factor, forget_bias, extra_shrinkage_exponent, linear_norm_gain, differential_output_rows, linear_output_rows):
    normed = rms_scale(tokens.astype(jnp.float32), input_norm_gain).astype(jnp.bfloat16)

    def project(matrix):
        return jnp.dot(normed, matrix, preferred_element_type=jnp.float32).astype(jnp.bfloat16)
    query_norm = rms_scale(project(differential_query).astype(jnp.float32).reshape(SEQUENCE_LENGTH, DA_HEADS, 2, HEAD), query_norm_gain).astype(jnp.bfloat16)
    key_norm = rms_scale(project(differential_key).astype(jnp.float32).reshape(SEQUENCE_LENGTH, DA_HEADS, 2, HEAD), key_norm_gain).astype(jnp.bfloat16)
    value_rows = project(differential_value).reshape(SEQUENCE_LENGTH, DA_HEADS, VDIM)
    attn_maps = attention_reference(query_norm, key_norm, value_rows, second_map_weight)
    attn_out = (rms_scale(attn_maps, differential_norm_gain) * OUT_SCALE).transpose(1, 0, 2).reshape(SEQUENCE_LENGTH, DA_HEADS * VDIM).astype(jnp.bfloat16)
    queries = project(linear_query).astype(jnp.float32).reshape(SEQUENCE_LENGTH, RECURRENT_LANES, RECURRENT_DIM) * RECURRENT_DIM ** (-0.5)
    keys_rows = project(linear_key).astype(jnp.float32).reshape(SEQUENCE_LENGTH, RECURRENT_LANES, RECURRENT_DIM)
    values_rows = project(linear_value).astype(jnp.float32).reshape(SEQUENCE_LENGTH, RECURRENT_LANES, GLA_DV)
    gated = jax.nn.silu(project(linear_output_gate).astype(jnp.float32)).reshape(SEQUENCE_LENGTH, RECURRENT_LANES, GLA_DV)
    low_rank = project(forget_down_factor)
    sigmoid_preactivation = jnp.dot(low_rank, forget_up_factor, preferred_element_type=jnp.float32) + forget_bias
    shrinkage_exponent = jax.nn.log_sigmoid(sigmoid_preactivation).reshape(SEQUENCE_LENGTH, RECURRENT_LANES, RECURRENT_DIM) / SOFTMAX_DIVISOR + extra_shrinkage_exponent[:, :, None]
    chain_full = chain_reference(queries, keys_rows, values_rows, shrinkage_exponent)
    chain_out = (rms_scale(chain_full, linear_norm_gain) * gated).reshape(SEQUENCE_LENGTH, RECURRENT_LANES * GLA_DV).astype(jnp.bfloat16)
    attn_width = DA_HEADS // N_TP * VDIM
    chain_width = RECURRENT_LANES // N_TP * GLA_DV
    summed = jnp.zeros((SEQUENCE_LENGTH, D), jnp.float32)
    for group_index in range(N_TP):
        attn_cols = attn_out[:, group_index * attn_width:(group_index + 1) * attn_width]
        chain_cols = chain_out[:, group_index * chain_width:(group_index + 1) * chain_width]
        group_term = jnp.dot(attn_cols, differential_output_rows[group_index * attn_width:(group_index + 1) * attn_width], preferred_element_type=jnp.float32)
        group_term = group_term + jnp.dot(chain_cols, linear_output_rows[group_index * chain_width:(group_index + 1) * chain_width], preferred_element_type=jnp.float32)
        summed = summed + lax.optimization_barrier(group_term.astype(jnp.bfloat16)).astype(jnp.float32)
    return summed.astype(jnp.bfloat16)
```

```python
import jax
import jax.numpy as jnp
from jax import lax
from jax.experimental import pallas as pl
from jax.experimental.pallas import tpu as pltpu
from jax.sharding import Mesh
from jax.sharding import PartitionSpec as P

F32 = jnp.float32
BF16 = jnp.bfloat16
HEAD = 64
VDIM = 128
BLOCK = 128
SUB = 16
GROUPS = 8
MEMBERS = 8
SP = ("far", "pair", "y")
TEAM = ("pair", "y")
SP_TP = ("far", "pair", "y", "tp")
RMS_EPS = 1e-06
NEG_LARGE = -1e30
NT = (((1,), (1,)), ((), ()))


def two_parts(x):
    high = x.astype(BF16).astype(F32)
    return high, (x - high).astype(BF16).astype(F32)


def three_parts(x):
    high, rest = x.astype(BF16).astype(F32), None
    middle = (x - high).astype(BF16).astype(F32)
    rest = ((x - high) - middle).astype(BF16).astype(F32)
    return high, middle, rest


def dot(a, b):
    return jnp.dot(a, b, preferred_element_type=F32)


def dot_nt(a, b):
    return lax.dot_general(a, b, NT, preferred_element_type=F32)


def iota(shape, dim):
    return lax.broadcasted_iota(jnp.int32, shape, dim)


def two_map_norm(values, gain):
    first = iota(values.shape, 1) < HEAD
    squares = values * values
    low = jnp.sum(jnp.where(first, squares, 0.0), axis=1, keepdims=True)
    high = jnp.sum(jnp.where(first, 0.0, squares), axis=1, keepdims=True)
    mean_sq = jnp.where(first, low, high) * (1.0 / HEAD)
    return values * lax.rsqrt(mean_sq + RMS_EPS) * jnp.concatenate([gain, gain], axis=1)


def project_kernel(
    rows_ref, gain_ref, dq_ref, dk_ref, dv_ref, lq_ref, lk_ref, lv_ref, lg_ref, down_ref, up_ref,
    bias_ref, shrink_ref, qgain_ref, kgain_ref,
    team_ref, kv_ref, local_ref, decayed_ref, gate_ref, scores_ref,
):
    rows = rows_ref[...].reshape(BLOCK, rows_ref.shape[-1]).astype(F32)
    mean_sq = jnp.mean(rows * rows, axis=1, keepdims=True)
    normed = (rows * lax.rsqrt(mean_sq + RMS_EPS) * gain_ref[...]).astype(BF16)

    def project(ref):
        return dot(normed, ref[...]).astype(BF16)

    query = two_map_norm(project(dq_ref).astype(F32), qgain_ref[...]).astype(BF16)
    query = query * jnp.asarray(HEAD**-0.5, BF16)
    key = two_map_norm(project(dk_ref).astype(F32), kgain_ref[...]).astype(BF16)
    kv_ref[0:BLOCK] = key
    kv_ref[BLOCK:] = project(dv_ref)
    gate = project(lg_ref).astype(F32)
    gate_ref[...] = gate * jax.nn.sigmoid(gate)

    low = project(down_ref)
    pre = dot(low, up_ref[...]) + bias_ref[...]
    log_sig = jnp.minimum(pre, 0.0) - jnp.log1p(jnp.exp(-jnp.abs(pre)))
    log_a = log_sig * (1.0 / 16.0) + shrink_ref[...]
    lower = (iota((BLOCK, BLOCK), 0) >= iota((BLOCK, BLOCK), 1)).astype(BF16)
    total = sum(dot(lower, part.astype(BF16)) for part in three_parts(log_a))

    lq = project(lq_ref).astype(F32) * HEAD**-0.5
    lk = project(lk_ref).astype(F32)
    lv = project(lv_ref)
    scores_ref[...] = jnp.zeros_like(scores_ref)
    for step in range(1, BLOCK // SUB):
        at = step * SUB
        border = total[at - 1 : at]
        q_part = lq[at : at + SUB] * jnp.exp(total[at : at + SUB] - border)
        k_part = lk[:at] * jnp.exp(border - total[:at])
        scores_ref[at : at + SUB, 0:at] = dot_nt(q_part.astype(BF16), k_part.astype(BF16))
    scores = scores_ref[...]
    row = iota((BLOCK, BLOCK), 0)
    distance = row - iota((BLOCK, BLOCK), 1)
    for shift in range(SUB):
        k_part = lk if shift == 0 else pltpu.roll(lk, shift, 0)
        if shift == 0:
            terms = lq * k_part
        else:
            terms = lq * k_part * jnp.exp(jnp.minimum(total - pltpu.roll(total, shift, 0), 0.0))
        column = jnp.sum(terms, axis=1, keepdims=True)
        here = (distance == shift) & (row % SUB >= shift)
        scores = jnp.where(here, column, scores)
    local_ref[...] = dot(scores.astype(BF16), lv)
    decayed_ref[...] = (lq * jnp.exp(total)).astype(BF16)

    k_end = lk * jnp.exp(total[BLOCK - 1 :] - total)
    flipped = jnp.concatenate([total, k_end], axis=1).T
    decay = jnp.broadcast_to(flipped[:HEAD, BLOCK - 1 :], (HEAD, VDIM))
    state = dot(flipped[HEAD:].astype(BF16), lv)
    state_parts = two_parts(state)
    decay_parts = two_parts(decay)
    for member in range(MEMBERS):
        own = slice(member * 8, member * 8 + 8)
        team_ref[member, 0:BLOCK] = query
        team_ref[member, BLOCK:] = jnp.concatenate(
            [part[own] for part in (*state_parts, *decay_parts)], axis=0
        ).astype(BF16)


def joined(block, at):
    return block[at : at + 8] + block[at + 8 : at + 16]


def group_kernel(team_ref, kv_ref, out_ref):
    state = jnp.zeros((8, VDIM), F32)
    decay = jnp.zeros((8, VDIM), F32)
    for member in range(MEMBERS):
        block = team_ref[member, BLOCK:].astype(F32)
        own = joined(block, 16)
        state = state * jnp.exp(own) + joined(block, 0)
        decay = decay + own
    tail = jnp.concatenate([*two_parts(state), *two_parts(decay)], axis=0).astype(BF16)
    kv = kv_ref[...]
    for group in range(GROUPS):
        out_ref[group, 0 : 2 * BLOCK] = kv
        out_ref[group, 2 * BLOCK :] = tail


def attend_kernel(place_ref, weight_ref, team_ref, far_ref, out_ref, key_ref, value_ref):
    group, member = place_ref[0], place_ref[1]
    second_weight = weight_ref[0, 0]
    for other in range(GROUPS):
        span = slice(other * BLOCK, (other + 1) * BLOCK)
        key_ref[span] = far_ref[other, 0:BLOCK]
        value_ref[span, 0:VDIM] = far_ref[other, BLOCK : 2 * BLOCK]
    value_ref[:, VDIM:] = jnp.ones((GROUPS * BLOCK, VDIM), BF16)

    cols = GROUPS * BLOCK
    column = iota((1, cols), 1)
    key_pos = (column // BLOCK * MEMBERS + member) * BLOCK + column % BLOCK
    lane = iota((BLOCK, VDIM), 1)
    logs = jnp.zeros((BLOCK, VDIM), F32)

    def one(index, logs):
        query_pos = (group * MEMBERS + index) * BLOCK + iota((BLOCK, 1), 0)
        causal = key_pos <= query_pos
        found = []
        for which in range(2):
            half = slice(which * HEAD, (which + 1) * HEAD)
            query = team_ref[index, 0:BLOCK, half]
            scores = dot_nt(query, key_ref[:, half])
            scores = jnp.where(causal, scores, NEG_LARGE)
            peak = jnp.max(scores, axis=1, keepdims=True)
            weights = jnp.exp(scores - peak).astype(BF16)
            both = dot(weights, value_ref[...])
            sums = both[:, VDIM:]
            found.append(both[:, :VDIM] / sums)
            logs = jnp.where(lane == 2 * index + which, peak + jnp.log(sums), logs)
        out_ref[index, 0:BLOCK] = found[0].astype(BF16)
        out_ref[index, BLOCK : 2 * BLOCK] = (found[0] - second_weight * found[1]).astype(BF16)
        return logs

    logs = lax.fori_loop(0, MEMBERS, one, logs)

    carried = jnp.zeros((8, VDIM), F32)
    for other in range(GROUPS):
        block = far_ref[other, 2 * BLOCK :].astype(F32)
        carried = jnp.where(
            other < group, carried * jnp.exp(joined(block, 16)) + joined(block, 0), carried
        )
    log_parts = three_parts(logs.T[: 2 * MEMBERS])
    for index in range(MEMBERS):
        pair = slice(2 * index, 2 * index + 2)
        tail = jnp.concatenate(
            [part[pair] for part in log_parts]
            + [jnp.zeros((10, VDIM), F32), *two_parts(carried)],
            axis=0,
        )
        out_ref[index, 2 * BLOCK :] = tail.astype(BF16)
        block = team_ref[index, BLOCK:].astype(F32)
        carried = carried * jnp.exp(joined(block, 16)) + joined(block, 0)


def finish_kernel(
    parts_ref, local_ref, decayed_ref, gate_ref, dgain_ref, lgain_ref, drows_ref, lrows_ref, out_ref
):
    logs, states = [[], []], []
    for member in range(MEMBERS):
        tail = parts_ref[member, 2 * BLOCK :].astype(F32)
        for which in range(2):
            logs[which].append(
                tail[which : which + 1] + tail[which + 2 : which + 3] + tail[which + 4 : which + 5]
            )
        states.append(tail[16:24] + tail[24:32])
    shares = []
    for which in range(2):
        stacked = jnp.concatenate(logs[which], axis=0)
        raised = jnp.exp(stacked - jnp.max(stacked, axis=0, keepdims=True))
        shares.append(raised / jnp.sum(raised, axis=0, keepdims=True))
    factors = jnp.concatenate(
        [shares[0] - shares[1], shares[1], jnp.zeros((BLOCK - 2 * MEMBERS, VDIM), F32)], axis=0
    ).T
    mixed = jnp.zeros((BLOCK, VDIM), F32)
    for member in range(MEMBERS):
        first = parts_ref[member, 0:BLOCK].astype(F32)
        gap = parts_ref[member, BLOCK : 2 * BLOCK].astype(F32)
        mixed = mixed + factors[:, member : member + 1] * first
        mixed = mixed + factors[:, MEMBERS + member : MEMBERS + member + 1] * gap
    mean_sq = jnp.mean(mixed * mixed, axis=1, keepdims=True)
    attn = (0.8 * (mixed * lax.rsqrt(mean_sq + RMS_EPS) * dgain_ref[...])).astype(BF16)

    state = jnp.concatenate(states, axis=0).astype(BF16)
    chain = local_ref[...] + dot(decayed_ref[...], state)
    mean_sq = jnp.mean(chain * chain, axis=1, keepdims=True)
    chain = (chain * lax.rsqrt(mean_sq + RMS_EPS) * lgain_ref[...] * gate_ref[...]).astype(BF16)
    out_ref[...] = (dot(attn, drows_ref[...]) + dot(chain, lrows_ref[...])).astype(BF16)


def call(kernel, outs, scratch=(), scalars=0, inputs=0):
    vmem = pl.BlockSpec(memory_space=pltpu.VMEM)
    smem = pl.BlockSpec(memory_space=pltpu.SMEM)
    return pl.pallas_call(
        kernel,
        in_specs=[smem] * scalars + [vmem] * inputs,
        out_specs=jax.tree.map(lambda _: vmem, outs),
        out_shape=outs,
        scratch_shapes=scratch,
        compiler_params=pltpu.CompilerParams(vmem_limit_bytes=48 * 1024 * 1024),
    )


def exchanged(blocks, axis):
    return lax.all_to_all(blocks, axis, split_axis=0, concat_axis=0, tiled=True)


def per_device(
    tokens, input_norm_gain, differential_query, differential_key, differential_value,
    query_norm_gain, key_norm_gain, second_map_weight, differential_norm_gain, linear_query,
    linear_key, linear_value, linear_output_gate, forget_down_factor, forget_up_factor,
    forget_bias, extra_shrinkage_exponent, linear_norm_gain, differential_output_rows,
    linear_output_rows,
):
    shape = jax.ShapeDtypeStruct
    copies = lax.axis_size("tp")
    rows = exchanged(jnp.broadcast_to(tokens, (copies, *tokens.shape)), "tp")
    place = jnp.stack([lax.axis_index("far"), lax.axis_index(TEAM)]).astype(jnp.int32)

    team, kv, local, decayed, gate = call(
        project_kernel,
        (
            shape((MEMBERS, BLOCK + 32, VDIM), BF16),
            shape((2 * BLOCK, VDIM), BF16),
            shape((BLOCK, VDIM), F32),
            shape((BLOCK, HEAD), BF16),
            shape((BLOCK, VDIM), F32),
        ),
        scratch=[pltpu.VMEM((BLOCK, BLOCK), F32)],
        inputs=15,
    )(
        rows, input_norm_gain.reshape(1, -1), differential_query, differential_key,
        differential_value, linear_query, linear_key, linear_value, linear_output_gate,
        forget_down_factor, forget_up_factor, forget_bias.reshape(1, -1),
        extra_shrinkage_exponent, query_norm_gain.reshape(1, -1), key_norm_gain.reshape(1, -1),
    )
    team = exchanged(team, TEAM)
    far = call(group_kernel, shape((GROUPS, 2 * BLOCK + 32, VDIM), BF16), inputs=2)(team, kv)
    far = exchanged(far, "far")
    parts = call(
        attend_kernel,
        shape((MEMBERS, 2 * BLOCK + 32, VDIM), BF16),
        scratch=[
            pltpu.VMEM((GROUPS * BLOCK, VDIM), BF16),
            pltpu.VMEM((GROUPS * BLOCK, 2 * VDIM), BF16),
        ],
        scalars=1,
        inputs=3,
    )(place, second_map_weight.reshape(1, 1), team, far)
    parts = exchanged(parts, TEAM)
    mixed = call(finish_kernel, shape((BLOCK, differential_output_rows.shape[1]), BF16), inputs=8)(
        parts, local, decayed, gate, differential_norm_gain.reshape(1, -1),
        linear_norm_gain.reshape(1, -1), differential_output_rows, linear_output_rows,
    )
    arrived = exchanged(mixed.reshape(copies, BLOCK // copies, -1), "tp")
    return arrived.astype(F32).sum(axis=0).astype(BF16)


def solution(mesh):
    torus = Mesh(
        mesh.devices.reshape(GROUPS, 2, 4, mesh.shape["tp"]), ("far", "pair", "y", "tp")
    )
    cols, lines = P(None, "tp"), P("tp", None)
    placed = (
        P(SP_TP, None), P(), cols, cols, cols, P(), P(), P("tp"), P(), cols, cols, cols, cols,
        P(), cols, P("tp"), P(SP, "tp"), P(), lines, lines,
    )
    return jax.shard_map(
        per_device, mesh=torus, in_specs=placed, out_specs=P(SP_TP, None), check_vma=False
    )
```

```python
import jax
import jax.numpy as jnp
from jax import lax
from jax.experimental import pallas as pl
from jax.experimental.pallas import tpu as pltpu
from jax.sharding import Mesh
from jax.sharding import PartitionSpec as P

F32 = jnp.float32
BF16 = jnp.bfloat16
HEAD = 64
VDIM = 128
BLOCK = 128
SUB = 16
GROUPS = 8
MEMBERS = 8
SP = ("far", "pair", "y")
TEAM = ("pair", "y")
TP = ("x", "core")
SP_TP = ("far", "pair", "y", "x", "core")
RMS_EPS = 1e-06
NEG_LARGE = -1e30
NT = (((1,), (1,)), ((), ()))


def two_parts(x):
    high = x.astype(BF16).astype(F32)
    return high, (x - high).astype(BF16).astype(F32)


def three_parts(x):
    high, rest = x.astype(BF16).astype(F32), None
    middle = (x - high).astype(BF16).astype(F32)
    rest = ((x - high) - middle).astype(BF16).astype(F32)
    return high, middle, rest


def dot(a, b):
    return jnp.dot(a, b, preferred_element_type=F32)


def dot_nt(a, b):
    return lax.dot_general(a, b, NT, preferred_element_type=F32)


def iota(shape, dim):
    return lax.broadcasted_iota(jnp.int32, shape, dim)


def two_map_norm(values, gain):
    first = iota(values.shape, 1) < HEAD
    squares = values * values
    low = jnp.sum(jnp.where(first, squares, 0.0), axis=1, keepdims=True)
    high = jnp.sum(jnp.where(first, 0.0, squares), axis=1, keepdims=True)
    mean_sq = jnp.where(first, low, high) * (1.0 / HEAD)
    return values * lax.rsqrt(mean_sq + RMS_EPS) * gain


def prepare_kernel(
    bias_ref, shrink_ref, qgain_ref, kgain_ref, dgain_ref, lgain_ref, gain_ref, up_ref,
    small_ref, shrunk_ref, ready_gain_ref, ready_up_ref,
):
    small_ref[0:1] = jnp.concatenate([qgain_ref[...]] * 2, axis=1)
    small_ref[1:2] = jnp.concatenate([kgain_ref[...]] * 2, axis=1)
    small_ref[2:3] = jnp.concatenate([bias_ref[...]] * 2, axis=1)
    small_ref[3:4] = dgain_ref[...]
    small_ref[4:5] = lgain_ref[...]
    small_ref[5:] = jnp.zeros((3, VDIM), F32)
    shrunk_ref[...] = jnp.broadcast_to(shrink_ref[...], shrunk_ref.shape).T
    ready_gain_ref[...] = gain_ref[...]
    ready_up_ref[...] = up_ref[...]


def project_kernel(
    rows_ref, gain_ref, dq_ref, lv_ref, lk_ref, down_ref, small_ref, shrunk_ref, up_ref,
    team_ref, normed_ref, lk_out_ref, lv_out_ref, total_ref,
):
    rows = jnp.concatenate(
        [rows_ref[core, chip] for chip in range(rows_ref.shape[1]) for core in range(2)], axis=0
    ).astype(F32)
    mean_sq = jnp.mean(rows * rows, axis=1, keepdims=True)
    normed = (rows * lax.rsqrt(mean_sq + RMS_EPS) * gain_ref[...]).astype(BF16)
    normed_ref[...] = normed

    lk = dot_nt(normed, lk_ref[...]).astype(BF16)
    low = dot_nt(normed, down_ref[...]).astype(BF16)
    lv = dot(normed, lv_ref[...]).astype(BF16)
    lk_out_ref[...] = lk
    lv_out_ref[...] = lv

    query = two_map_norm(dot(normed, dq_ref[...]).astype(BF16).astype(F32), small_ref[0:1])
    query = query.astype(BF16) * jnp.asarray(HEAD**-0.5, BF16)

    pre = dot(low, up_ref[...]) + small_ref[2:3, 0:HEAD]
    log_sig = jnp.minimum(pre, 0.0) - jnp.log1p(jnp.exp(-jnp.abs(pre)))
    log_a = log_sig * (1.0 / 16.0) + shrunk_ref[:, 0:HEAD]
    lower = (iota((BLOCK, BLOCK), 0) >= iota((BLOCK, BLOCK), 1)).astype(BF16)
    total = sum(dot(lower, piece.astype(BF16)) for piece in three_parts(log_a))

    total_ref[...] = total
    k_end = lk.astype(F32) * jnp.exp(total[BLOCK - 1 :] - total)
    flipped = jnp.concatenate([total, k_end], axis=1).T
    decay = jnp.broadcast_to(flipped[:HEAD, BLOCK - 1 :], (HEAD, VDIM))
    state = dot(flipped[HEAD:].astype(BF16), lv)
    state_parts = two_parts(state)
    decay_parts = two_parts(decay)
    for member in range(MEMBERS):
        own = slice(member * 8, member * 8 + 8)
        team_ref[member, 0:BLOCK] = query
        team_ref[member, BLOCK:] = jnp.concatenate(
            [piece[own] for piece in (*state_parts, *decay_parts)], axis=0
        ).astype(BF16)


def key_value_kernel(normed_ref, dk_ref, dv_ref, small_ref, kv_ref):
    normed = normed_ref[...]
    key = two_map_norm(dot(normed, dk_ref[...]).astype(BF16).astype(F32), small_ref[1:2])
    kv_ref[0:BLOCK] = key.astype(BF16)
    kv_ref[BLOCK:] = dot(normed, dv_ref[...]).astype(BF16)


def local_kernel(
    normed_ref, lg_ref, lq_ref, lk_ref, lv_ref, total_ref, local_ref, decayed_ref, gate_ref,
    scores_ref,
):
    gate = dot(normed_ref[...], lg_ref[...]).astype(BF16).astype(F32)
    gate_ref[...] = gate * jax.nn.sigmoid(gate)
    lq = dot_nt(normed_ref[...], lq_ref[...]).astype(BF16).astype(F32) * HEAD**-0.5
    lk = lk_ref[...].astype(F32)
    lv = lv_ref[...]
    total = total_ref[...]
    scores_ref[...] = jnp.zeros_like(scores_ref)
    for step in range(1, BLOCK // SUB):
        at = step * SUB
        border = total[at - 1 : at]
        q_part = lq[at : at + SUB] * jnp.exp(total[at : at + SUB] - border)
        k_part = lk[:at] * jnp.exp(border - total[:at])
        scores_ref[at : at + SUB, 0:at] = dot_nt(q_part.astype(BF16), k_part.astype(BF16))
    scores = scores_ref[...]
    row = iota((BLOCK, BLOCK), 0)
    distance = row - iota((BLOCK, BLOCK), 1)
    for shift in range(SUB):
        k_part = lk if shift == 0 else pltpu.roll(lk, shift, 0)
        if shift == 0:
            terms = lq * k_part
        else:
            terms = lq * k_part * jnp.exp(jnp.minimum(total - pltpu.roll(total, shift, 0), 0.0))
        column = jnp.sum(terms, axis=1, keepdims=True)
        here = (distance == shift) & (row % SUB >= shift)
        scores = jnp.where(here, column, scores)
    local_ref[...] = dot(scores.astype(BF16), lv)
    decayed_ref[...] = (lq * jnp.exp(total)).astype(BF16)


def joined(block, at):
    return block[at : at + 8] + block[at + 8 : at + 16]


def group_kernel(team_ref, kv_ref, out_ref):
    state = jnp.zeros((8, VDIM), F32)
    decay = jnp.zeros((8, VDIM), F32)
    for member in range(MEMBERS):
        block = team_ref[member, BLOCK:].astype(F32)
        own = joined(block, 16)
        state = state * jnp.exp(own) + joined(block, 0)
        decay = decay + own
    tail = jnp.concatenate([*two_parts(state), *two_parts(decay)], axis=0).astype(BF16)
    out_ref[0 : 2 * BLOCK] = kv_ref[...]
    out_ref[2 * BLOCK :] = tail


def attend_kernel(
    place_ref, weight_ref, team_ref, far_ref, out_ref, query_ref, key_ref, value_ref, logs_ref
):
    group, member = place_ref[0], place_ref[1]
    second_weight = weight_ref[0, 0]
    for other in range(GROUPS):
        span = slice(other * BLOCK, (other + 1) * BLOCK)
        query_ref[span] = team_ref[other, 0:BLOCK]
        key_ref[span] = far_ref[other, 0:BLOCK]
        value_ref[span, 0:VDIM] = far_ref[other, BLOCK : 2 * BLOCK]
    value_ref[:, VDIM:] = jnp.ones((GROUPS * BLOCK, VDIM), BF16)

    column = iota((1, 2 * BLOCK), 1)
    key_pos = (column // BLOCK * MEMBERS + member) * BLOCK + column % BLOCK
    lane = iota((BLOCK, VDIM), 1)
    logs_ref[...] = jnp.zeros_like(logs_ref)

    def attend(blocks):
        cols, open_cols = blocks * BLOCK, (blocks - 2) * BLOCK
        last_pos = key_pos + (blocks - 2) * MEMBERS * BLOCK
        batch = {2: 8, 4: 4}.get(blocks, 2)
        rows = batch * BLOCK

        def one(step, _):
            start = pl.multiple_of(step * rows, rows)
            causal = last_pos <= group * MEMBERS * BLOCK + start + iota((rows, 1), 0)
            found, logs = [], []
            for which in range(2):
                half = slice(which * HEAD, (which + 1) * HEAD)
                query = query_ref[pl.ds(start, rows), half]
                scores = dot_nt(query, key_ref[open_cols:cols, half])
                scores = jnp.where(causal, scores, NEG_LARGE)
                if open_cols:
                    scores = jnp.concatenate(
                        [dot_nt(query, key_ref[0:open_cols, half]), scores], axis=1
                    )
                peak = jnp.max(scores, axis=1, keepdims=True)
                weights = jnp.exp(scores - peak).astype(BF16)
                both = dot(weights, value_ref[0:cols])
                sums = both[:, VDIM:]
                found.append(both[:, :VDIM] / sums)
                logs.append(peak + jnp.log(sums))
            gap = found[0] - second_weight * found[1]
            total = logs_ref[...]
            for near in range(batch):
                index = step * batch + near
                part = slice(near * BLOCK, (near + 1) * BLOCK)
                out_ref[index, 0:BLOCK] = found[0][part].astype(BF16)
                out_ref[index, BLOCK : 2 * BLOCK] = gap[part].astype(BF16)
                for which in range(2):
                    total = jnp.where(lane == 2 * index + which, logs[which][part], total)
            logs_ref[...] = total
            return _

        if batch == MEMBERS:
            one(0, 0)
        else:
            lax.fori_loop(0, MEMBERS // batch, one, 0)

    for blocks in range(2, GROUPS + 1, 2):
        pl.when(group // 2 == blocks // 2 - 1)(lambda blocks=blocks: attend(blocks))
    logs = logs_ref[...]

    carried = jnp.zeros((8, VDIM), F32)
    for other in range(GROUPS):
        block = far_ref[other, 2 * BLOCK :].astype(F32)
        carried = jnp.where(
            other < group, carried * jnp.exp(joined(block, 16)) + joined(block, 0), carried
        )
    log_parts = three_parts(logs.T[: 2 * MEMBERS])
    for index in range(MEMBERS):
        pair = slice(2 * index, 2 * index + 2)
        tail = jnp.concatenate(
            [part[pair] for part in log_parts]
            + [jnp.zeros((10, VDIM), F32), *two_parts(carried)],
            axis=0,
        )
        out_ref[index, 2 * BLOCK :] = tail.astype(BF16)
        block = team_ref[index, BLOCK:].astype(F32)
        carried = carried * jnp.exp(joined(block, 16)) + joined(block, 0)


def finish_kernel(
    parts_ref, local_ref, decayed_ref, gate_ref, small_ref, drows_ref, lrows_ref, out_ref
):
    logs, states = [[], []], []
    for member in range(MEMBERS):
        tail = parts_ref[member, 2 * BLOCK :].astype(F32)
        for which in range(2):
            logs[which].append(
                tail[which : which + 1] + tail[which + 2 : which + 3] + tail[which + 4 : which + 5]
            )
        states.append(tail[16:24] + tail[24:32])
    shares = []
    for which in range(2):
        stacked = jnp.concatenate(logs[which], axis=0)
        raised = jnp.exp(stacked - jnp.max(stacked, axis=0, keepdims=True))
        shares.append(raised / jnp.sum(raised, axis=0, keepdims=True))
    factors = jnp.concatenate(
        [shares[0] - shares[1], shares[1], jnp.zeros((BLOCK - 2 * MEMBERS, VDIM), F32)], axis=0
    ).T
    mixed = jnp.zeros((BLOCK, VDIM), F32)
    for member in range(MEMBERS):
        first = parts_ref[member, 0:BLOCK].astype(F32)
        gap = parts_ref[member, BLOCK : 2 * BLOCK].astype(F32)
        mixed = mixed + factors[:, member : member + 1] * first
        mixed = mixed + factors[:, MEMBERS + member : MEMBERS + member + 1] * gap
    mean_sq = jnp.mean(mixed * mixed, axis=1, keepdims=True)
    attn = (0.8 * (mixed * lax.rsqrt(mean_sq + RMS_EPS) * small_ref[3:4])).astype(BF16)

    state = jnp.concatenate(states, axis=0).astype(BF16)
    chain = local_ref[...] + dot(decayed_ref[...], state)
    mean_sq = jnp.mean(chain * chain, axis=1, keepdims=True)
    chain = (chain * lax.rsqrt(mean_sq + RMS_EPS) * small_ref[4:5] * gate_ref[...]).astype(BF16)
    out_ref[...] = (dot(attn, drows_ref[...]) + dot(chain, lrows_ref[...])).astype(BF16)


def call(kernel, outs, scratch=(), scalars=0, inputs=0):
    vmem = pl.BlockSpec(memory_space=pltpu.VMEM)
    smem = pl.BlockSpec(memory_space=pltpu.SMEM)
    return pl.pallas_call(
        kernel,
        in_specs=[smem] * scalars + [vmem] * inputs,
        out_specs=jax.tree.map(lambda _: vmem, outs),
        out_shape=outs,
        scratch_shapes=scratch,
        compiler_params=pltpu.CompilerParams(vmem_limit_bytes=48 * 2**20),
    )


def exchanged(blocks, axis):
    return lax.all_to_all(blocks, axis, split_axis=0, concat_axis=0, tiled=True)


def per_device(
    tokens, input_norm_gain, differential_query, differential_key, differential_value,
    query_norm_gain, key_norm_gain, second_map_weight, differential_norm_gain, linear_query,
    linear_key, linear_value, linear_output_gate, forget_down_factor, forget_up_factor,
    forget_bias, extra_shrinkage_exponent, linear_norm_gain, differential_output_rows,
    linear_output_rows,
):
    shape = jax.ShapeDtypeStruct
    copies = lax.axis_size(TP)
    rows = exchanged(jnp.broadcast_to(tokens, (copies // 2, *tokens.shape)), "x")
    rows = lax.all_gather(rows, "core")
    place = jnp.stack([lax.axis_index("far"), lax.axis_index(TEAM)]).astype(jnp.int32)

    features = tokens.shape[1]
    small, shrunk, gain, up = call(
        prepare_kernel,
        (
            shape((8, VDIM), F32),
            shape((BLOCK, VDIM), F32),
            shape((1, features), F32),
            shape(forget_up_factor.shape, BF16),
        ),
        inputs=8,
    )(
        forget_bias.reshape(1, -1), extra_shrinkage_exponent.reshape(1, -1),
        query_norm_gain.reshape(1, -1), key_norm_gain.reshape(1, -1),
        differential_norm_gain.reshape(1, -1), linear_norm_gain.reshape(1, -1),
        input_norm_gain.reshape(1, -1), forget_up_factor,
    )
    team, normed, lk, lv, total = call(
        project_kernel,
        (
            shape((MEMBERS, BLOCK + 32, VDIM), BF16),
            shape((BLOCK, features), BF16),
            shape((BLOCK, HEAD), BF16),
            shape((BLOCK, VDIM), BF16),
            shape((BLOCK, HEAD), F32),
        ),
        inputs=9,
    )(
        rows, gain, differential_query, linear_value, linear_key.T, forget_down_factor.T, small,
        shrunk, up,
    )
    kv = call(key_value_kernel, shape((2 * BLOCK, VDIM), BF16), inputs=4)(
        normed, differential_key, differential_value, small
    )
    local, decayed, gate = call(
        local_kernel,
        (
            shape((BLOCK, VDIM), F32),
            shape((BLOCK, HEAD), BF16),
            shape((BLOCK, VDIM), F32),
        ),
        scratch=[pltpu.VMEM((BLOCK, BLOCK), F32)],
        inputs=6,
    )(normed, linear_output_gate, linear_query.T, lk, lv, total)
    team = exchanged(team, TEAM)
    far = call(group_kernel, shape((2 * BLOCK + 32, VDIM), BF16), inputs=2)(team, kv)
    far = lax.all_gather(far, "far")
    parts = call(
        attend_kernel,
        shape((MEMBERS, 2 * BLOCK + 32, VDIM), BF16),
        scratch=[
            pltpu.VMEM((MEMBERS * BLOCK, VDIM), BF16),
            pltpu.VMEM((GROUPS * BLOCK, VDIM), BF16),
            pltpu.VMEM((GROUPS * BLOCK, 2 * VDIM), BF16),
            pltpu.VMEM((BLOCK, VDIM), F32),
        ],
        scalars=1,
        inputs=3,
    )(place, second_map_weight.reshape(1, 1), team, far)
    parts = exchanged(parts, TEAM)
    mixed = call(finish_kernel, shape((BLOCK, differential_output_rows.shape[1]), BF16), inputs=7)(
        parts, local, decayed, gate, small, differential_output_rows, linear_output_rows
    )
    arrived = exchanged(mixed.reshape(copies, BLOCK // copies, -1), TP)
    return arrived.astype(F32).sum(axis=0).astype(BF16)


def solution(mesh):
    torus = Mesh(
        mesh.devices.reshape(GROUPS, 2, 4, mesh.shape["tp"] // 2, 2),
        ("far", "pair", "y", "x", "core"),
    )
    cols, lines = P(None, TP), P(TP, None)
    placed = (
        P(SP_TP, None), P(), cols, cols, cols, P(), P(), P(TP), P(), cols, cols, cols, cols,
        P(), cols, P(TP), P(SP, TP), P(), lines, lines,
    )
    return jax.shard_map(
        per_device, mesh=torus, in_specs=placed, out_specs=P(SP_TP, None), check_vma=False
    )
```

```python
import jax
import jax.numpy as jnp
from jax import lax
from jax.experimental import pallas as pl
from jax.experimental.pallas import tpu as pltpu
from jax.sharding import Mesh
from jax.sharding import PartitionSpec as P

F32 = jnp.float32
BF16 = jnp.bfloat16
HEAD = 64
VDIM = 128
BLOCK = 128
SUB = 16
GROUPS = 8
MEMBERS = 8
SP = ("far", "pair", "y")
TEAM = ("pair", "y")
TP = ("x", "core")
SP_TP = ("far", "pair", "y", "x", "core")
RMS_EPS = 1e-06
NEG_LARGE = -1e30
NT = (((1,), (1,)), ((), ()))


def two_parts(x):
    high = x.astype(BF16).astype(F32)
    return high, (x - high).astype(BF16).astype(F32)


def three_parts(x):
    high, rest = x.astype(BF16).astype(F32), None
    middle = (x - high).astype(BF16).astype(F32)
    rest = ((x - high) - middle).astype(BF16).astype(F32)
    return high, middle, rest


def dot(a, b):
    return jnp.dot(a, b, preferred_element_type=F32)


def dot_nt(a, b):
    return lax.dot_general(a, b, NT, preferred_element_type=F32)


def iota(shape, dim):
    return lax.broadcasted_iota(jnp.int32, shape, dim)


def two_map_norm(values, gain):
    first = iota(values.shape, 1) < HEAD
    squares = values * values
    low = jnp.sum(jnp.where(first, squares, 0.0), axis=1, keepdims=True)
    high = jnp.sum(jnp.where(first, 0.0, squares), axis=1, keepdims=True)
    mean_sq = jnp.where(first, low, high) * (1.0 / HEAD)
    return values * lax.rsqrt(mean_sq + RMS_EPS) * gain


def prepare_kernel(
    bias_ref, shrink_ref, qgain_ref, kgain_ref, dgain_ref, lgain_ref, gain_ref, up_ref,
    small_ref, shrunk_ref, ready_gain_ref, ready_up_ref,
):
    small_ref[0:1] = jnp.concatenate([qgain_ref[...]] * 2, axis=1)
    small_ref[1:2] = jnp.concatenate([kgain_ref[...]] * 2, axis=1)
    small_ref[2:3] = jnp.concatenate([bias_ref[...]] * 2, axis=1)
    small_ref[3:4] = dgain_ref[...]
    small_ref[4:5] = lgain_ref[...]
    small_ref[5:] = jnp.zeros((3, VDIM), F32)
    shrunk_ref[...] = jnp.broadcast_to(shrink_ref[...], shrunk_ref.shape).T
    ready_gain_ref[...] = gain_ref[...]
    ready_up_ref[...] = up_ref[...]


def project_kernel(
    rows_ref, gain_ref, dq_ref, lv_ref, lk_ref, down_ref, small_ref, shrunk_ref, up_ref,
    team_ref, normed_ref, lk_out_ref, lv_out_ref, total_ref,
):
    rows = jnp.concatenate(
        [rows_ref[core, chip] for chip in range(rows_ref.shape[1]) for core in range(2)], axis=0
    ).astype(F32)
    mean_sq = jnp.mean(rows * rows, axis=1, keepdims=True)
    normed = (rows * lax.rsqrt(mean_sq + RMS_EPS) * gain_ref[...]).astype(BF16)
    normed_ref[...] = normed

    lk = dot_nt(normed, lk_ref[...]).astype(BF16)
    low = dot_nt(normed, down_ref[...]).astype(BF16)
    lv = dot(normed, lv_ref[...]).astype(BF16)
    lk_out_ref[...] = lk
    lv_out_ref[...] = lv

    query = two_map_norm(dot(normed, dq_ref[...]).astype(BF16).astype(F32), small_ref[0:1])
    query = query.astype(BF16) * jnp.asarray(HEAD**-0.5, BF16)

    pre = dot(low, up_ref[...]) + small_ref[2:3, 0:HEAD]
    log_sig = jnp.minimum(pre, 0.0) - jnp.log1p(jnp.exp(-jnp.abs(pre)))
    log_a = log_sig * (1.0 / 16.0) + shrunk_ref[:, 0:HEAD]
    lower = (iota((BLOCK, BLOCK), 0) >= iota((BLOCK, BLOCK), 1)).astype(BF16)
    total = sum(dot(lower, piece.astype(BF16)) for piece in three_parts(log_a))

    total_ref[...] = total
    k_end = lk.astype(F32) * jnp.exp(total[BLOCK - 1 :] - total)
    flipped = jnp.concatenate([total, k_end], axis=1).T
    decay = jnp.broadcast_to(flipped[:HEAD, BLOCK - 1 :], (HEAD, VDIM))
    state = dot(flipped[HEAD:].astype(BF16), lv)
    state_parts = two_parts(state)
    decay_parts = two_parts(decay)
    for member in range(MEMBERS):
        own = slice(member * 8, member * 8 + 8)
        team_ref[member, 0:BLOCK] = query
        team_ref[member, BLOCK:] = jnp.concatenate(
            [piece[own] for piece in (*state_parts, *decay_parts)], axis=0
        ).astype(BF16)


def local_kernel(
    normed_ref, dk_ref, dv_ref, lg_ref, lq_ref, lk_ref, lv_ref, total_ref, small_ref,
    kv_ref, local_ref, decayed_ref, gate_ref, scores_ref,
):
    normed = normed_ref[...]
    key = two_map_norm(dot(normed, dk_ref[...]).astype(BF16).astype(F32), small_ref[1:2])
    kv_ref[0:BLOCK] = key.astype(BF16)
    kv_ref[BLOCK:] = dot(normed, dv_ref[...]).astype(BF16)
    gate = dot(normed, lg_ref[...]).astype(BF16).astype(F32)
    gate_ref[...] = gate * jax.nn.sigmoid(gate)
    lq = dot_nt(normed, lq_ref[...]).astype(BF16).astype(F32) * HEAD**-0.5
    lk = lk_ref[...].astype(F32)
    lv = lv_ref[...]
    total = total_ref[...]
    scores_ref[...] = jnp.zeros_like(scores_ref)
    for step in range(1, BLOCK // SUB):
        at = step * SUB
        border = total[at - 1 : at]
        q_part = lq[at : at + SUB] * jnp.exp(total[at : at + SUB] - border)
        k_part = lk[:at] * jnp.exp(border - total[:at])
        scores_ref[at : at + SUB, 0:at] = dot_nt(q_part.astype(BF16), k_part.astype(BF16))
    scores = scores_ref[...]
    row = iota((BLOCK, BLOCK), 0)
    distance = row - iota((BLOCK, BLOCK), 1)
    for shift in range(SUB):
        k_part = lk if shift == 0 else pltpu.roll(lk, shift, 0)
        if shift == 0:
            terms = lq * k_part
        else:
            terms = lq * k_part * jnp.exp(jnp.minimum(total - pltpu.roll(total, shift, 0), 0.0))
        column = jnp.sum(terms, axis=1, keepdims=True)
        here = (distance == shift) & (row % SUB >= shift)
        scores = jnp.where(here, column, scores)
    local_ref[...] = dot(scores.astype(BF16), lv)
    decayed_ref[...] = (lq * jnp.exp(total)).astype(BF16)


def joined(block, at):
    return block[at : at + 8] + block[at + 8 : at + 16]


def group_kernel(team_ref, kv_ref, out_ref):
    state = jnp.zeros((8, VDIM), F32)
    decay = jnp.zeros((8, VDIM), F32)
    for member in range(MEMBERS):
        block = team_ref[member, BLOCK:].astype(F32)
        own = joined(block, 16)
        state = state * jnp.exp(own) + joined(block, 0)
        decay = decay + own
    tail = jnp.concatenate([*two_parts(state), *two_parts(decay)], axis=0).astype(BF16)
    out_ref[0 : 2 * BLOCK] = kv_ref[...]
    out_ref[2 * BLOCK :] = tail


def attend_kernel(
    place_ref, weight_ref, team_ref, far_ref, out_ref, query_ref, key_ref, value_ref, logs_ref
):
    group, member = place_ref[0], place_ref[1]
    second_weight = weight_ref[0, 0]
    for other in range(GROUPS):
        span = slice(other * BLOCK, (other + 1) * BLOCK)
        query_ref[span] = team_ref[other, 0:BLOCK]
        key_ref[span] = far_ref[other, 0:BLOCK]
        value_ref[span, 0:VDIM] = far_ref[other, BLOCK : 2 * BLOCK]
    value_ref[:, VDIM:] = jnp.ones((GROUPS * BLOCK, VDIM), BF16)

    column = iota((1, 2 * BLOCK), 1)
    key_pos = (column // BLOCK * MEMBERS + member) * BLOCK + column % BLOCK
    lane = iota((BLOCK, VDIM), 1)
    logs_ref[...] = jnp.zeros_like(logs_ref)

    def attend(blocks):
        cols, open_cols = blocks * BLOCK, (blocks - 2) * BLOCK
        last_pos = key_pos + (blocks - 2) * MEMBERS * BLOCK
        batch = {2: 8, 4: 8, 6: 4}.get(blocks, 2)
        rows = batch * BLOCK

        def one(step, _):
            start = pl.multiple_of(step * rows, rows)
            causal = last_pos <= group * MEMBERS * BLOCK + start + iota((rows, 1), 0)
            found, logs = [], []
            for which in range(2):
                half = slice(which * HEAD, (which + 1) * HEAD)
                query = query_ref[pl.ds(start, rows), half]
                scores = dot_nt(query, key_ref[open_cols:cols, half])
                scores = jnp.where(causal, scores, NEG_LARGE)
                if open_cols:
                    scores = jnp.concatenate(
                        [dot_nt(query, key_ref[0:open_cols, half]), scores], axis=1
                    )
                peak = jnp.max(scores, axis=1, keepdims=True)
                weights = jnp.exp(scores - peak).astype(BF16)
                both = dot(weights, value_ref[0:cols])
                sums = both[:, VDIM:]
                found.append(both[:, :VDIM] / sums)
                logs.append(peak + jnp.log(sums))
            gap = found[0] - second_weight * found[1]
            total = logs_ref[...]
            for near in range(batch):
                index = step * batch + near
                part = slice(near * BLOCK, (near + 1) * BLOCK)
                out_ref[index, 0:BLOCK] = found[0][part].astype(BF16)
                out_ref[index, BLOCK : 2 * BLOCK] = gap[part].astype(BF16)
                for which in range(2):
                    total = jnp.where(lane == 2 * index + which, logs[which][part], total)
            logs_ref[...] = total
            return _

        if batch == MEMBERS:
            one(0, 0)
        else:
            lax.fori_loop(0, MEMBERS // batch, one, 0, unroll=True)

    for blocks in range(2, GROUPS + 1, 2):
        pl.when(group // 2 == blocks // 2 - 1)(lambda blocks=blocks: attend(blocks))
    logs = logs_ref[...]

    carried = jnp.zeros((8, VDIM), F32)
    for other in range(GROUPS):
        block = far_ref[other, 2 * BLOCK :].astype(F32)
        carried = jnp.where(
            other < group, carried * jnp.exp(joined(block, 16)) + joined(block, 0), carried
        )
    log_parts = three_parts(logs.T[: 2 * MEMBERS])
    for index in range(MEMBERS):
        pair = slice(2 * index, 2 * index + 2)
        tail = jnp.concatenate(
            [part[pair] for part in log_parts]
            + [jnp.zeros((10, VDIM), F32), *two_parts(carried)],
            axis=0,
        )
        out_ref[index, 2 * BLOCK :] = tail.astype(BF16)
        block = team_ref[index, BLOCK:].astype(F32)
        carried = carried * jnp.exp(joined(block, 16)) + joined(block, 0)


def finish_kernel(
    parts_ref, local_ref, decayed_ref, gate_ref, small_ref, drows_ref, lrows_ref, out_ref
):
    logs, states = [[], []], []
    for member in range(MEMBERS):
        tail = parts_ref[member, 2 * BLOCK :].astype(F32)
        for which in range(2):
            logs[which].append(
                tail[which : which + 1] + tail[which + 2 : which + 3] + tail[which + 4 : which + 5]
            )
        states.append(tail[16:24] + tail[24:32])
    shares = []
    for which in range(2):
        stacked = jnp.concatenate(logs[which], axis=0)
        raised = jnp.exp(stacked - jnp.max(stacked, axis=0, keepdims=True))
        shares.append(raised / jnp.sum(raised, axis=0, keepdims=True))
    factors = jnp.concatenate(
        [shares[0] - shares[1], shares[1], jnp.zeros((BLOCK - 2 * MEMBERS, VDIM), F32)], axis=0
    ).T
    mixed = jnp.zeros((BLOCK, VDIM), F32)
    for member in range(MEMBERS):
        first = parts_ref[member, 0:BLOCK].astype(F32)
        gap = parts_ref[member, BLOCK : 2 * BLOCK].astype(F32)
        mixed = mixed + factors[:, member : member + 1] * first
        mixed = mixed + factors[:, MEMBERS + member : MEMBERS + member + 1] * gap
    mean_sq = jnp.mean(mixed * mixed, axis=1, keepdims=True)
    attn = (0.8 * (mixed * lax.rsqrt(mean_sq + RMS_EPS) * small_ref[3:4])).astype(BF16)

    state = jnp.concatenate(states, axis=0).astype(BF16)
    chain = local_ref[...] + dot(decayed_ref[...], state)
    mean_sq = jnp.mean(chain * chain, axis=1, keepdims=True)
    chain = (chain * lax.rsqrt(mean_sq + RMS_EPS) * small_ref[4:5] * gate_ref[...]).astype(BF16)
    out_ref[...] = (dot(attn, drows_ref[...]) + dot(chain, lrows_ref[...])).astype(BF16)


def call(kernel, outs, scratch=(), scalars=0, inputs=0):
    vmem = pl.BlockSpec(memory_space=pltpu.VMEM)
    smem = pl.BlockSpec(memory_space=pltpu.SMEM)
    return pl.pallas_call(
        kernel,
        in_specs=[smem] * scalars + [vmem] * inputs,
        out_specs=jax.tree.map(lambda _: vmem, outs),
        out_shape=outs,
        scratch_shapes=scratch,
        compiler_params=pltpu.CompilerParams(vmem_limit_bytes=48 * 2**20),
    )


def exchanged(blocks, axis):
    return lax.all_to_all(blocks, axis, split_axis=0, concat_axis=0, tiled=True)


def per_device(
    tokens, input_norm_gain, differential_query, differential_key, differential_value,
    query_norm_gain, key_norm_gain, second_map_weight, differential_norm_gain, linear_query,
    linear_key, linear_value, linear_output_gate, forget_down_factor, forget_up_factor,
    forget_bias, extra_shrinkage_exponent, linear_norm_gain, differential_output_rows,
    linear_output_rows,
):
    shape = jax.ShapeDtypeStruct
    copies = lax.axis_size(TP)
    rows = exchanged(jnp.broadcast_to(tokens, (copies // 2, *tokens.shape)), "x")
    rows = lax.all_gather(rows, "core")
    place = jnp.stack([lax.axis_index("far"), lax.axis_index(TEAM)]).astype(jnp.int32)

    features = tokens.shape[1]
    small, shrunk, gain, up = call(
        prepare_kernel,
        (
            shape((8, VDIM), F32),
            shape((BLOCK, VDIM), F32),
            shape((1, features), F32),
            shape(forget_up_factor.shape, BF16),
        ),
        inputs=8,
    )(
        forget_bias.reshape(1, -1), extra_shrinkage_exponent.reshape(1, -1),
        query_norm_gain.reshape(1, -1), key_norm_gain.reshape(1, -1),
        differential_norm_gain.reshape(1, -1), linear_norm_gain.reshape(1, -1),
        input_norm_gain.reshape(1, -1), forget_up_factor,
    )
    team, normed, lk, lv, total = call(
        project_kernel,
        (
            shape((MEMBERS, BLOCK + 32, VDIM), BF16),
            shape((BLOCK, features), BF16),
            shape((BLOCK, HEAD), BF16),
            shape((BLOCK, VDIM), BF16),
            shape((BLOCK, HEAD), F32),
        ),
        inputs=9,
    )(
        rows, gain, differential_query, linear_value, linear_key.T, forget_down_factor.T, small,
        shrunk, up,
    )
    kv, local, decayed, gate = call(
        local_kernel,
        (
            shape((2 * BLOCK, VDIM), BF16),
            shape((BLOCK, VDIM), F32),
            shape((BLOCK, HEAD), BF16),
            shape((BLOCK, VDIM), F32),
        ),
        scratch=[pltpu.VMEM((BLOCK, BLOCK), F32)],
        inputs=9,
    )(
        normed, differential_key, differential_value, linear_output_gate, linear_query.T, lk, lv,
        total, small,
    )
    team = exchanged(team, TEAM)
    far = call(group_kernel, shape((2 * BLOCK + 32, VDIM), BF16), inputs=2)(team, kv)
    far = lax.all_gather(far, "far")
    parts = call(
        attend_kernel,
        shape((MEMBERS, 2 * BLOCK + 32, VDIM), BF16),
        scratch=[
            pltpu.VMEM((MEMBERS * BLOCK, VDIM), BF16),
            pltpu.VMEM((GROUPS * BLOCK, VDIM), BF16),
            pltpu.VMEM((GROUPS * BLOCK, 2 * VDIM), BF16),
            pltpu.VMEM((BLOCK, VDIM), F32),
        ],
        scalars=1,
        inputs=3,
    )(place, second_map_weight.reshape(1, 1), team, far)
    parts = exchanged(parts, TEAM)
    mixed = call(finish_kernel, shape((BLOCK, differential_output_rows.shape[1]), BF16), inputs=7)(
        parts, local, decayed, gate, small, differential_output_rows, linear_output_rows
    )
    arrived = exchanged(mixed.reshape(copies, BLOCK // copies, -1), TP)
    return arrived.astype(F32).sum(axis=0).astype(BF16)


def solution(mesh):
    torus = Mesh(
        mesh.devices.reshape(GROUPS, 2, 4, mesh.shape["tp"] // 2, 2),
        ("far", "pair", "y", "x", "core"),
    )
    cols, lines = P(None, TP), P(TP, None)
    placed = (
        P(SP_TP, None), P(), cols, cols, cols, P(), P(), P(TP), P(), cols, cols, cols, cols,
        P(), cols, P(TP), P(SP, TP), P(), lines, lines,
    )
    return jax.shard_map(
        per_device, mesh=torus, in_specs=placed, out_specs=P(SP_TP, None), check_vma=False
    )
```

```python
import jax
import jax.numpy as jnp
from jax import lax
from jax.experimental import pallas as pl
from jax.experimental.pallas import tpu as pltpu
from jax.sharding import Mesh
from jax.sharding import PartitionSpec as P

F32 = jnp.float32
BF16 = jnp.bfloat16
HEAD = 64
VDIM = 128
BLOCK = 128
SUB = 16
GROUPS = 8
MEMBERS = 8
SP = ("far", "pair", "y")
TEAM = ("pair", "y")
TP = ("x", "core")
SP_TP = ("far", "pair", "y", "x", "core")
RMS_EPS = 1e-06
NEG_LARGE = -1e30
NT = (((1,), (1,)), ((), ()))


def two_parts(x):
    high = x.astype(BF16).astype(F32)
    return high, (x - high).astype(BF16).astype(F32)


def three_parts(x):
    high, rest = x.astype(BF16).astype(F32), None
    middle = (x - high).astype(BF16).astype(F32)
    rest = ((x - high) - middle).astype(BF16).astype(F32)
    return high, middle, rest


def dot(a, b):
    return jnp.dot(a, b, preferred_element_type=F32)


def dot_nt(a, b):
    return lax.dot_general(a, b, NT, preferred_element_type=F32)


def iota(shape, dim):
    return lax.broadcasted_iota(jnp.int32, shape, dim)


def two_map_norm(values, gain):
    first = iota(values.shape, 1) < HEAD
    squares = values * values
    low = jnp.sum(jnp.where(first, squares, 0.0), axis=1, keepdims=True)
    high = jnp.sum(jnp.where(first, 0.0, squares), axis=1, keepdims=True)
    mean_sq = jnp.where(first, low, high) * (1.0 / HEAD)
    return values * lax.rsqrt(mean_sq + RMS_EPS) * gain


def prepare_kernel(
    bias_ref, shrink_ref, qgain_ref, kgain_ref, dgain_ref, lgain_ref, gain_ref, up_ref,
    small_ref, shrunk_ref, ready_gain_ref, ready_up_ref,
):
    small_ref[0:1] = jnp.concatenate([qgain_ref[...]] * 2, axis=1)
    small_ref[1:2] = jnp.concatenate([kgain_ref[...]] * 2, axis=1)
    small_ref[2:3] = jnp.concatenate([bias_ref[...]] * 2, axis=1)
    small_ref[3:4] = dgain_ref[...]
    small_ref[4:5] = lgain_ref[...]
    small_ref[5:] = jnp.zeros((3, VDIM), F32)
    shrunk_ref[...] = jnp.broadcast_to(shrink_ref[...], shrunk_ref.shape).T
    ready_gain_ref[...] = gain_ref[...]
    ready_up_ref[...] = up_ref[...]


def copy_kernel(tokens_ref, copies_ref):
    tokens = tokens_ref[...]
    for chip in range(copies_ref.shape[0]):
        copies_ref[chip] = tokens


def project_kernel(
    rows_ref, gain_ref, dq_ref, lv_ref, lk_ref, down_ref, small_ref, shrunk_ref, up_ref,
    team_ref, normed_ref, lk_out_ref, lv_out_ref, total_ref,
):
    rows = jnp.concatenate(
        [rows_ref[core, chip] for chip in range(rows_ref.shape[1]) for core in range(2)], axis=0
    ).astype(F32)
    mean_sq = jnp.mean(rows * rows, axis=1, keepdims=True)
    normed = (rows * lax.rsqrt(mean_sq + RMS_EPS) * gain_ref[...]).astype(BF16)
    normed_ref[...] = normed

    lk = dot_nt(normed, lk_ref[...]).astype(BF16)
    low = dot_nt(normed, down_ref[...]).astype(BF16)
    lv = dot(normed, lv_ref[...]).astype(BF16)
    lk_out_ref[...] = lk
    lv_out_ref[...] = lv

    query = two_map_norm(dot(normed, dq_ref[...]).astype(BF16).astype(F32), small_ref[0:1])
    query = query.astype(BF16) * jnp.asarray(HEAD**-0.5, BF16)

    pre = dot(low, up_ref[...]) + small_ref[2:3, 0:HEAD]
    log_sig = jnp.minimum(pre, 0.0) - jnp.log1p(jnp.exp(-jnp.abs(pre)))
    log_a = log_sig * (1.0 / 16.0) + shrunk_ref[:, 0:HEAD]
    lower = (iota((BLOCK, BLOCK), 0) >= iota((BLOCK, BLOCK), 1)).astype(BF16)
    total = sum(dot(lower, piece.astype(BF16)) for piece in three_parts(log_a))

    total_ref[...] = total
    k_end = lk.astype(F32) * jnp.exp(total[BLOCK - 1 :] - total)
    flipped = jnp.concatenate([total, k_end], axis=1).T
    decay = jnp.broadcast_to(flipped[:HEAD, BLOCK - 1 :], (HEAD, VDIM))
    state = dot(flipped[HEAD:].astype(BF16), lv)
    state_parts = two_parts(state)
    decay_parts = two_parts(decay)
    for member in range(MEMBERS):
        own = slice(member * 8, member * 8 + 8)
        team_ref[member, 0:BLOCK] = query
        team_ref[member, BLOCK:] = jnp.concatenate(
            [piece[own] for piece in (*state_parts, *decay_parts)], axis=0
        ).astype(BF16)


def local_kernel(
    normed_ref, dk_ref, dv_ref, lg_ref, lq_ref, lk_ref, lv_ref, total_ref, small_ref,
    kv_ref, local_ref, decayed_ref, gate_ref, scores_ref,
):
    normed = normed_ref[...]
    key = two_map_norm(dot(normed, dk_ref[...]).astype(BF16).astype(F32), small_ref[1:2])
    kv_ref[0:BLOCK] = key.astype(BF16)
    kv_ref[BLOCK:] = dot(normed, dv_ref[...]).astype(BF16)
    gate = dot(normed, lg_ref[...]).astype(BF16).astype(F32)
    gate_ref[...] = gate * jax.nn.sigmoid(gate)
    lq = dot_nt(normed, lq_ref[...]).astype(BF16).astype(F32) * HEAD**-0.5
    lk = lk_ref[...].astype(F32)
    lv = lv_ref[...]
    total = total_ref[...]
    scores_ref[...] = jnp.zeros_like(scores_ref)
    for step in range(1, BLOCK // SUB):
        at = step * SUB
        border = total[at - 1 : at]
        q_part = lq[at : at + SUB] * jnp.exp(total[at : at + SUB] - border)
        k_part = lk[:at] * jnp.exp(border - total[:at])
        scores_ref[at : at + SUB, 0:at] = dot_nt(q_part.astype(BF16), k_part.astype(BF16))
    scores = scores_ref[...]
    row = iota((BLOCK, BLOCK), 0)
    distance = row - iota((BLOCK, BLOCK), 1)
    for shift in range(SUB):
        k_part = lk if shift == 0 else pltpu.roll(lk, shift, 0)
        if shift == 0:
            terms = lq * k_part
        else:
            terms = lq * k_part * jnp.exp(jnp.minimum(total - pltpu.roll(total, shift, 0), 0.0))
        column = jnp.sum(terms, axis=1, keepdims=True)
        here = (distance == shift) & (row % SUB >= shift)
        scores = jnp.where(here, column, scores)
    local_ref[...] = dot(scores.astype(BF16), lv)
    decayed_ref[...] = (lq * jnp.exp(total)).astype(BF16)


def joined(block, at):
    return block[at : at + 8] + block[at + 8 : at + 16]


def group_kernel(team_ref, kv_ref, out_ref):
    state = jnp.zeros((8, VDIM), F32)
    decay = jnp.zeros((8, VDIM), F32)
    for member in range(MEMBERS):
        block = team_ref[member, BLOCK:].astype(F32)
        own = joined(block, 16)
        state = state * jnp.exp(own) + joined(block, 0)
        decay = decay + own
    tail = jnp.concatenate([*two_parts(state), *two_parts(decay)], axis=0).astype(BF16)
    out_ref[0 : 2 * BLOCK] = kv_ref[...]
    out_ref[2 * BLOCK :] = tail


def attend_kernel(
    place_ref, weight_ref, team_ref, far_ref, out_ref, query_ref, key_ref, value_ref, logs_ref
):
    group, member = place_ref[0], place_ref[1]
    second_weight = weight_ref[0, 0]
    for other in range(GROUPS):
        span = slice(other * BLOCK, (other + 1) * BLOCK)
        query_ref[span] = team_ref[other, 0:BLOCK]
        key_ref[span] = far_ref[other, 0:BLOCK]
        value_ref[span, 0:VDIM] = far_ref[other, BLOCK : 2 * BLOCK]
    value_ref[:, VDIM:] = jnp.ones((GROUPS * BLOCK, VDIM), BF16)

    column = iota((1, 2 * BLOCK), 1)
    key_pos = (column // BLOCK * MEMBERS + member) * BLOCK + column % BLOCK
    lane = iota((BLOCK, VDIM), 1)
    logs_ref[...] = jnp.zeros_like(logs_ref)

    def attend(blocks):
        cols, open_cols = blocks * BLOCK, (blocks - 2) * BLOCK
        last_pos = key_pos + (blocks - 2) * MEMBERS * BLOCK
        batch = {2: 8, 4: 8, 6: 4}.get(blocks, 2)
        rows = batch * BLOCK

        def one(step, _):
            start = pl.multiple_of(step * rows, rows)
            causal = last_pos <= group * MEMBERS * BLOCK + start + iota((rows, 1), 0)
            found, logs = [], []
            for which in range(2):
                half = slice(which * HEAD, (which + 1) * HEAD)
                query = query_ref[pl.ds(start, rows), half]
                scores = dot_nt(query, key_ref[open_cols:cols, half])
                scores = jnp.where(causal, scores, NEG_LARGE)
                if open_cols:
                    scores = jnp.concatenate(
                        [dot_nt(query, key_ref[0:open_cols, half]), scores], axis=1
                    )
                peak = jnp.max(scores, axis=1, keepdims=True)
                weights = jnp.exp(scores - peak).astype(BF16)
                both = dot(weights, value_ref[0:cols])
                sums = both[:, VDIM:]
                found.append(both[:, :VDIM] / sums)
                logs.append(peak + jnp.log(sums))
            gap = found[0] - second_weight * found[1]
            total = logs_ref[...]
            for near in range(batch):
                index = step * batch + near
                part = slice(near * BLOCK, (near + 1) * BLOCK)
                out_ref[index, 0:BLOCK] = found[0][part].astype(BF16)
                out_ref[index, BLOCK : 2 * BLOCK] = gap[part].astype(BF16)
                for which in range(2):
                    total = jnp.where(lane == 2 * index + which, logs[which][part], total)
            logs_ref[...] = total
            return _

        if batch == MEMBERS:
            one(0, 0)
        else:
            lax.fori_loop(0, MEMBERS // batch, one, 0, unroll=True)

    for blocks in range(2, GROUPS + 1, 2):
        pl.when(group // 2 == blocks // 2 - 1)(lambda blocks=blocks: attend(blocks))
    logs = logs_ref[...]

    carried = jnp.zeros((8, VDIM), F32)
    for other in range(GROUPS):
        block = far_ref[other, 2 * BLOCK :].astype(F32)
        carried = jnp.where(
            other < group, carried * jnp.exp(joined(block, 16)) + joined(block, 0), carried
        )
    log_parts = three_parts(logs.T[: 2 * MEMBERS])
    for index in range(MEMBERS):
        pair = slice(2 * index, 2 * index + 2)
        tail = jnp.concatenate(
            [part[pair] for part in log_parts]
            + [jnp.zeros((10, VDIM), F32), *two_parts(carried)],
            axis=0,
        )
        out_ref[index, 2 * BLOCK :] = tail.astype(BF16)
        block = team_ref[index, BLOCK:].astype(F32)
        carried = carried * jnp.exp(joined(block, 16)) + joined(block, 0)


def finish_kernel(
    parts_ref, local_ref, decayed_ref, gate_ref, small_ref, drows_ref, lrows_ref, out_ref
):
    logs, states = [[], []], []
    for member in range(MEMBERS):
        tail = parts_ref[member, 2 * BLOCK :].astype(F32)
        for which in range(2):
            logs[which].append(
                tail[which : which + 1] + tail[which + 2 : which + 3] + tail[which + 4 : which + 5]
            )
        states.append(tail[16:24] + tail[24:32])
    shares = []
    for which in range(2):
        stacked = jnp.concatenate(logs[which], axis=0)
        raised = jnp.exp(stacked - jnp.max(stacked, axis=0, keepdims=True))
        shares.append(raised / jnp.sum(raised, axis=0, keepdims=True))
    factors = jnp.concatenate(
        [shares[0] - shares[1], shares[1], jnp.zeros((BLOCK - 2 * MEMBERS, VDIM), F32)], axis=0
    ).T
    mixed = jnp.zeros((BLOCK, VDIM), F32)
    for member in range(MEMBERS):
        first = parts_ref[member, 0:BLOCK].astype(F32)
        gap = parts_ref[member, BLOCK : 2 * BLOCK].astype(F32)
        mixed = mixed + factors[:, member : member + 1] * first
        mixed = mixed + factors[:, MEMBERS + member : MEMBERS + member + 1] * gap
    mean_sq = jnp.mean(mixed * mixed, axis=1, keepdims=True)
    attn = (0.8 * (mixed * lax.rsqrt(mean_sq + RMS_EPS) * small_ref[3:4])).astype(BF16)

    state = jnp.concatenate(states, axis=0).astype(BF16)
    chain = local_ref[...] + dot(decayed_ref[...], state)
    mean_sq = jnp.mean(chain * chain, axis=1, keepdims=True)
    chain = (chain * lax.rsqrt(mean_sq + RMS_EPS) * small_ref[4:5] * gate_ref[...]).astype(BF16)
    out_ref[...] = (dot(attn, drows_ref[...]) + dot(chain, lrows_ref[...])).astype(BF16)


def call(kernel, outs, scratch=(), scalars=0, inputs=0):
    vmem = pl.BlockSpec(memory_space=pltpu.VMEM)
    smem = pl.BlockSpec(memory_space=pltpu.SMEM)
    return pl.pallas_call(
        kernel,
        in_specs=[smem] * scalars + [vmem] * inputs,
        out_specs=jax.tree.map(lambda _: vmem, outs),
        out_shape=outs,
        scratch_shapes=scratch,
        compiler_params=pltpu.CompilerParams(vmem_limit_bytes=48 * 2**20),
    )


def exchanged(blocks, axis):
    return lax.all_to_all(blocks, axis, split_axis=0, concat_axis=0, tiled=True)


def per_device(
    tokens, input_norm_gain, differential_query, differential_key, differential_value,
    query_norm_gain, key_norm_gain, second_map_weight, differential_norm_gain, linear_query,
    linear_key, linear_value, linear_output_gate, forget_down_factor, forget_up_factor,
    forget_bias, extra_shrinkage_exponent, linear_norm_gain, differential_output_rows,
    linear_output_rows,
):
    shape = jax.ShapeDtypeStruct
    copies = lax.axis_size(TP)
    rows = call(copy_kernel, shape((copies // 2, *tokens.shape), BF16), inputs=1)(tokens)
    rows = exchanged(rows, "x")
    rows = lax.all_gather(rows, "core")
    place = jnp.stack([lax.axis_index("far"), lax.axis_index(TEAM)]).astype(jnp.int32)

    features = tokens.shape[1]
    small, shrunk, gain, up = call(
        prepare_kernel,
        (
            shape((8, VDIM), F32),
            shape((BLOCK, VDIM), F32),
            shape((1, features), F32),
            shape(forget_up_factor.shape, BF16),
        ),
        inputs=8,
    )(
        forget_bias.reshape(1, -1), extra_shrinkage_exponent.reshape(1, -1),
        query_norm_gain.reshape(1, -1), key_norm_gain.reshape(1, -1),
        differential_norm_gain.reshape(1, -1), linear_norm_gain.reshape(1, -1),
        input_norm_gain.reshape(1, -1), forget_up_factor,
    )
    team, normed, lk, lv, total = call(
        project_kernel,
        (
            shape((MEMBERS, BLOCK + 32, VDIM), BF16),
            shape((BLOCK, features), BF16),
            shape((BLOCK, HEAD), BF16),
            shape((BLOCK, VDIM), BF16),
            shape((BLOCK, HEAD), F32),
        ),
        inputs=9,
    )(
        rows, gain, differential_query, linear_value, linear_key.T, forget_down_factor.T, small,
        shrunk, up,
    )
    kv, local, decayed, gate = call(
        local_kernel,
        (
            shape((2 * BLOCK, VDIM), BF16),
            shape((BLOCK, VDIM), F32),
            shape((BLOCK, HEAD), BF16),
            shape((BLOCK, VDIM), F32),
        ),
        scratch=[pltpu.VMEM((BLOCK, BLOCK), F32)],
        inputs=9,
    )(
        normed, differential_key, differential_value, linear_output_gate, linear_query.T, lk, lv,
        total, small,
    )
    team = exchanged(team, TEAM)
    far = call(group_kernel, shape((2 * BLOCK + 32, VDIM), BF16), inputs=2)(team, kv)
    far = lax.all_gather(far, "far")
    parts = call(
        attend_kernel,
        shape((MEMBERS, 2 * BLOCK + 32, VDIM), BF16),
        scratch=[
            pltpu.VMEM((MEMBERS * BLOCK, VDIM), BF16),
            pltpu.VMEM((GROUPS * BLOCK, VDIM), BF16),
            pltpu.VMEM((GROUPS * BLOCK, 2 * VDIM), BF16),
            pltpu.VMEM((BLOCK, VDIM), F32),
        ],
        scalars=1,
        inputs=3,
    )(place, second_map_weight.reshape(1, 1), team, far)
    parts = exchanged(parts, TEAM)
    mixed = call(finish_kernel, shape((BLOCK, differential_output_rows.shape[1]), BF16), inputs=7)(
        parts, local, decayed, gate, small, differential_output_rows, linear_output_rows
    )
    arrived = exchanged(mixed.reshape(copies, BLOCK // copies, -1), TP)
    return arrived.astype(F32).sum(axis=0).astype(BF16)


def solution(mesh):
    torus = Mesh(
        mesh.devices.reshape(GROUPS, 2, 4, mesh.shape["tp"] // 2, 2),
        ("far", "pair", "y", "x", "core"),
    )
    cols, lines = P(None, TP), P(TP, None)
    placed = (
        P(SP_TP, None), P(), cols, cols, cols, P(), P(), P(TP), P(), cols, cols, cols, cols,
        P(), cols, P(TP), P(SP, TP), P(), lines, lines,
    )
    return jax.shard_map(
        per_device, mesh=torus, in_specs=placed, out_specs=P(SP_TP, None), check_vma=False
    )
```

```python
import jax
import jax.numpy as jnp
from jax import lax
from jax.experimental import pallas as pl
from jax.experimental.pallas import tpu as pltpu
from jax.sharding import Mesh
from jax.sharding import PartitionSpec as P

F32 = jnp.float32
BF16 = jnp.bfloat16
HEAD = 64
VDIM = 128
BLOCK = 128
SUB = 16
GROUPS = 8
MEMBERS = 8
SP = ("far", "pair", "y")
TEAM = ("pair", "y")
TP = ("x", "core")
SP_TP = ("far", "pair", "y", "x", "core")
RMS_EPS = 1e-06
NEG_LARGE = -1e30
NT = (((1,), (1,)), ((), ()))


def two_parts(x):
    high = x.astype(BF16).astype(F32)
    return high, (x - high).astype(BF16).astype(F32)


def three_parts(x):
    high, rest = x.astype(BF16).astype(F32), None
    middle = (x - high).astype(BF16).astype(F32)
    rest = ((x - high) - middle).astype(BF16).astype(F32)
    return high, middle, rest


def dot(a, b):
    return jnp.dot(a, b, preferred_element_type=F32)


def dot_nt(a, b):
    return lax.dot_general(a, b, NT, preferred_element_type=F32)


def iota(shape, dim):
    return lax.broadcasted_iota(jnp.int32, shape, dim)


def two_map_norm(values, gain):
    first = iota(values.shape, 1) < HEAD
    squares = values * values
    low = jnp.sum(jnp.where(first, squares, 0.0), axis=1, keepdims=True)
    high = jnp.sum(jnp.where(first, 0.0, squares), axis=1, keepdims=True)
    mean_sq = jnp.where(first, low, high) * (1.0 / HEAD)
    return values * lax.rsqrt(mean_sq + RMS_EPS) * gain


def prepare_kernel(
    bias_ref, shrink_ref, qgain_ref, kgain_ref, dgain_ref, lgain_ref, gain_ref, up_ref,
    small_ref, shrunk_ref, ready_gain_ref, ready_up_ref,
):
    small_ref[0:1] = jnp.concatenate([qgain_ref[...]] * 2, axis=1)
    small_ref[1:2] = jnp.concatenate([kgain_ref[...]] * 2, axis=1)
    small_ref[2:3] = jnp.concatenate([bias_ref[...]] * 2, axis=1)
    small_ref[3:4] = dgain_ref[...]
    small_ref[4:5] = lgain_ref[...]
    small_ref[5:] = jnp.zeros((3, VDIM), F32)
    shrunk_ref[...] = jnp.broadcast_to(shrink_ref[...], shrunk_ref.shape).T
    ready_gain_ref[...] = gain_ref[...]
    ready_up_ref[...] = up_ref[...]


def copy_kernel(tokens_ref, copies_ref):
    tokens = tokens_ref[...]
    for chip in range(copies_ref.shape[0]):
        copies_ref[chip] = tokens


def project_kernel(
    rows_ref, gain_ref, dq_ref, lv_ref, lk_ref, down_ref, small_ref, shrunk_ref, up_ref,
    team_ref, normed_ref, lk_out_ref, lv_out_ref, total_ref,
):
    rows = jnp.concatenate(
        [rows_ref[core, chip] for chip in range(rows_ref.shape[1]) for core in range(2)], axis=0
    ).astype(F32)
    mean_sq = jnp.mean(rows * rows, axis=1, keepdims=True)
    normed = (rows * lax.rsqrt(mean_sq + RMS_EPS) * gain_ref[...]).astype(BF16)
    normed_ref[...] = normed

    lk = dot_nt(normed, lk_ref[...]).astype(BF16)
    low = dot_nt(normed, down_ref[...]).astype(BF16)
    lv = dot(normed, lv_ref[...]).astype(BF16)
    lk_out_ref[...] = lk
    lv_out_ref[...] = lv

    query = two_map_norm(dot(normed, dq_ref[...]).astype(BF16).astype(F32), small_ref[0:1])
    query = query.astype(BF16) * jnp.asarray(HEAD**-0.5, BF16)

    pre = dot(low, up_ref[...]) + small_ref[2:3, 0:HEAD]
    log_sig = jnp.minimum(pre, 0.0) - jnp.log1p(jnp.exp(-jnp.abs(pre)))
    log_a = log_sig * (1.0 / 16.0) + shrunk_ref[:, 0:HEAD]
    lower = (iota((BLOCK, BLOCK), 0) >= iota((BLOCK, BLOCK), 1)).astype(BF16)
    total = sum(dot(lower, piece.astype(BF16)) for piece in three_parts(log_a))

    total_ref[...] = total
    k_end = lk.astype(F32) * jnp.exp(total[BLOCK - 1 :] - total)
    flipped = jnp.concatenate([total, k_end], axis=1).T
    decay = jnp.broadcast_to(flipped[:HEAD, BLOCK - 1 :], (HEAD, VDIM))
    state = dot(flipped[HEAD:].astype(BF16), lv)
    state_parts = two_parts(state)
    decay_parts = two_parts(decay)
    for member in range(MEMBERS):
        own = slice(member * 8, member * 8 + 8)
        team_ref[member, 0:BLOCK] = query
        team_ref[member, BLOCK:] = jnp.concatenate(
            [piece[own] for piece in (*state_parts, *decay_parts)], axis=0
        ).astype(BF16)


def local_kernel(
    normed_ref, dk_ref, dv_ref, lg_ref, lq_ref, lk_ref, lv_ref, total_ref, small_ref,
    kv_ref, local_ref, decayed_ref, gate_ref, scores_ref,
):
    normed = normed_ref[...]
    key = two_map_norm(dot(normed, dk_ref[...]).astype(BF16).astype(F32), small_ref[1:2])
    kv_ref[0:BLOCK] = key.astype(BF16)
    kv_ref[BLOCK:] = dot(normed, dv_ref[...]).astype(BF16)
    gate = dot(normed, lg_ref[...]).astype(BF16).astype(F32)
    gate_ref[...] = gate * jax.nn.sigmoid(gate)
    lq = dot_nt(normed, lq_ref[...]).astype(BF16).astype(F32) * HEAD**-0.5
    lk = lk_ref[...].astype(F32)
    lv = lv_ref[...]
    total = total_ref[...]
    scores_ref[...] = jnp.zeros_like(scores_ref)
    for step in range(1, BLOCK // SUB):
        at = step * SUB
        border = total[at - 1 : at]
        q_part = lq[at : at + SUB] * jnp.exp(total[at : at + SUB] - border)
        k_part = lk[:at] * jnp.exp(border - total[:at])
        scores_ref[at : at + SUB, 0:at] = dot_nt(q_part.astype(BF16), k_part.astype(BF16))
    scores = scores_ref[...]
    row = iota((BLOCK, BLOCK), 0)
    distance = row - iota((BLOCK, BLOCK), 1)
    for shift in range(SUB):
        k_part = lk if shift == 0 else pltpu.roll(lk, shift, 0)
        if shift == 0:
            terms = lq * k_part
        else:
            terms = lq * k_part * jnp.exp(jnp.minimum(total - pltpu.roll(total, shift, 0), 0.0))
        column = jnp.sum(terms, axis=1, keepdims=True)
        here = (distance == shift) & (row % SUB >= shift)
        scores = jnp.where(here, column, scores)
    local_ref[...] = dot(scores.astype(BF16), lv)
    decayed_ref[...] = (lq * jnp.exp(total)).astype(BF16)


def joined(block, at):
    return block[at : at + 8] + block[at + 8 : at + 16]


def group_kernel(team_ref, kv_ref, out_ref):
    state = jnp.zeros((8, VDIM), F32)
    decay = jnp.zeros((8, VDIM), F32)
    for member in range(MEMBERS):
        block = team_ref[member, BLOCK:].astype(F32)
        own = joined(block, 16)
        state = state * jnp.exp(own) + joined(block, 0)
        decay = decay + own
    tail = jnp.concatenate([*two_parts(state), *two_parts(decay)], axis=0).astype(BF16)
    out_ref[0 : 2 * BLOCK] = kv_ref[...]
    out_ref[2 * BLOCK :] = tail


def attend_kernel(
    place_ref, weight_ref, team_ref, far_ref, out_ref, query_ref, key_ref, value_ref, logs_ref
):
    group, member = place_ref[0], place_ref[1]
    second_weight = weight_ref[0, 0]
    for other in range(GROUPS):
        span = slice(other * BLOCK, (other + 1) * BLOCK)
        query_ref[span] = team_ref[other, 0:BLOCK]
        key_ref[span] = far_ref[other, 0:BLOCK]
        value_ref[span, 0:VDIM] = far_ref[other, BLOCK : 2 * BLOCK]
    value_ref[:, VDIM:] = jnp.ones((GROUPS * BLOCK, VDIM), BF16)

    column = iota((1, 2 * BLOCK), 1)
    key_pos = (column // BLOCK * MEMBERS + member) * BLOCK + column % BLOCK
    lane = iota((BLOCK, VDIM), 1)
    logs_ref[...] = jnp.zeros_like(logs_ref)

    def attend(blocks):
        cols, open_cols = blocks * BLOCK, (blocks - 2) * BLOCK
        last_pos = key_pos + (blocks - 2) * MEMBERS * BLOCK
        batch = {2: 8, 4: 8, 6: 4}.get(blocks, 2)
        rows = batch * BLOCK

        def one(step, _):
            start = pl.multiple_of(step * rows, rows)
            causal = last_pos <= group * MEMBERS * BLOCK + start + iota((rows, 1), 0)
            found, logs = [], []
            for which in range(2):
                half = slice(which * HEAD, (which + 1) * HEAD)
                query = query_ref[pl.ds(start, rows), half]
                scores = dot_nt(query, key_ref[open_cols:cols, half])
                scores = jnp.where(causal, scores, NEG_LARGE)
                if open_cols:
                    scores = jnp.concatenate(
                        [dot_nt(query, key_ref[0:open_cols, half]), scores], axis=1
                    )
                peak = jnp.max(scores, axis=1, keepdims=True)
                weights = jnp.exp(scores - peak).astype(BF16)
                both = dot(weights, value_ref[0:cols])
                sums = both[:, VDIM:]
                found.append(both[:, :VDIM] / sums)
                logs.append(peak + jnp.log(sums))
            gap = found[0] - second_weight * found[1]
            total = logs_ref[...]
            for near in range(batch):
                index = step * batch + near
                part = slice(near * BLOCK, (near + 1) * BLOCK)
                out_ref[index, 0:BLOCK] = found[0][part].astype(BF16)
                out_ref[index, BLOCK : 2 * BLOCK] = gap[part].astype(BF16)
                for which in range(2):
                    total = jnp.where(lane == 2 * index + which, logs[which][part], total)
            logs_ref[...] = total
            return _

        if batch == MEMBERS:
            one(0, 0)
        else:
            lax.fori_loop(0, MEMBERS // batch, one, 0, unroll=True)

    for blocks in range(2, GROUPS + 1, 2):
        pl.when(group // 2 == blocks // 2 - 1)(lambda blocks=blocks: attend(blocks))
    logs = logs_ref[...]

    carried = jnp.zeros((8, VDIM), F32)
    for other in range(GROUPS):
        block = far_ref[other, 2 * BLOCK :].astype(F32)
        carried = jnp.where(
            other < group, carried * jnp.exp(joined(block, 16)) + joined(block, 0), carried
        )
    log_parts = three_parts(logs.T[: 2 * MEMBERS])
    for index in range(MEMBERS):
        pair = slice(2 * index, 2 * index + 2)
        tail = jnp.concatenate(
            [part[pair] for part in log_parts] + [jnp.zeros((2, VDIM), F32), carried],
            axis=0,
        )
        out_ref[index, 2 * BLOCK :] = tail.astype(BF16)
        block = team_ref[index, BLOCK:].astype(F32)
        carried = carried * jnp.exp(joined(block, 16)) + joined(block, 0)


def finish_kernel(
    parts_ref, local_ref, decayed_ref, gate_ref, small_ref, drows_ref, lrows_ref, out_ref
):
    logs, states = [[], []], []
    for member in range(MEMBERS):
        tail = parts_ref[member, 2 * BLOCK :].astype(F32)
        for which in range(2):
            logs[which].append(
                tail[which : which + 1] + tail[which + 2 : which + 3] + tail[which + 4 : which + 5]
            )
        states.append(tail[8:16])
    shares = []
    for which in range(2):
        stacked = jnp.concatenate(logs[which], axis=0)
        raised = jnp.exp(stacked - jnp.max(stacked, axis=0, keepdims=True))
        shares.append(raised / jnp.sum(raised, axis=0, keepdims=True))
    factors = jnp.concatenate(
        [shares[0] - shares[1], shares[1], jnp.zeros((BLOCK - 2 * MEMBERS, VDIM), F32)], axis=0
    ).T
    mixed = jnp.zeros((BLOCK, VDIM), F32)
    for member in range(MEMBERS):
        first = parts_ref[member, 0:BLOCK].astype(F32)
        gap = parts_ref[member, BLOCK : 2 * BLOCK].astype(F32)
        mixed = mixed + factors[:, member : member + 1] * first
        mixed = mixed + factors[:, MEMBERS + member : MEMBERS + member + 1] * gap
    mean_sq = jnp.mean(mixed * mixed, axis=1, keepdims=True)
    attn = (0.8 * (mixed * lax.rsqrt(mean_sq + RMS_EPS) * small_ref[3:4])).astype(BF16)

    state = jnp.concatenate(states, axis=0).astype(BF16)
    chain = local_ref[...] + dot(decayed_ref[...], state)
    mean_sq = jnp.mean(chain * chain, axis=1, keepdims=True)
    chain = (chain * lax.rsqrt(mean_sq + RMS_EPS) * small_ref[4:5] * gate_ref[...]).astype(BF16)
    out_ref[...] = (dot(attn, drows_ref[...]) + dot(chain, lrows_ref[...])).astype(BF16)


def call(kernel, outs, scratch=(), scalars=0, inputs=0):
    vmem = pl.BlockSpec(memory_space=pltpu.VMEM)
    smem = pl.BlockSpec(memory_space=pltpu.SMEM)
    return pl.pallas_call(
        kernel,
        in_specs=[smem] * scalars + [vmem] * inputs,
        out_specs=jax.tree.map(lambda _: vmem, outs),
        out_shape=outs,
        scratch_shapes=scratch,
        compiler_params=pltpu.CompilerParams(vmem_limit_bytes=48 * 2**20),
    )


def exchanged(blocks, axis):
    return lax.all_to_all(blocks, axis, split_axis=0, concat_axis=0, tiled=True)


def per_device(
    tokens, input_norm_gain, differential_query, differential_key, differential_value,
    query_norm_gain, key_norm_gain, second_map_weight, differential_norm_gain, linear_query,
    linear_key, linear_value, linear_output_gate, forget_down_factor, forget_up_factor,
    forget_bias, extra_shrinkage_exponent, linear_norm_gain, differential_output_rows,
    linear_output_rows,
):
    shape = jax.ShapeDtypeStruct
    copies = lax.axis_size(TP)
    rows = call(copy_kernel, shape((copies // 2, *tokens.shape), BF16), inputs=1)(tokens)
    rows = exchanged(rows, "x")
    rows = lax.all_gather(rows, "core")
    place = jnp.stack([lax.axis_index("far"), lax.axis_index(TEAM)]).astype(jnp.int32)

    features = tokens.shape[1]
    small, shrunk, gain, up = call(
        prepare_kernel,
        (
            shape((8, VDIM), F32),
            shape((BLOCK, VDIM), F32),
            shape((1, features), F32),
            shape(forget_up_factor.shape, BF16),
        ),
        inputs=8,
    )(
        forget_bias.reshape(1, -1), extra_shrinkage_exponent.reshape(1, -1),
        query_norm_gain.reshape(1, -1), key_norm_gain.reshape(1, -1),
        differential_norm_gain.reshape(1, -1), linear_norm_gain.reshape(1, -1),
        input_norm_gain.reshape(1, -1), forget_up_factor,
    )
    team, normed, lk, lv, total = call(
        project_kernel,
        (
            shape((MEMBERS, BLOCK + 32, VDIM), BF16),
            shape((BLOCK, features), BF16),
            shape((BLOCK, HEAD), BF16),
            shape((BLOCK, VDIM), BF16),
            shape((BLOCK, HEAD), F32),
        ),
        inputs=9,
    )(
        rows, gain, differential_query, linear_value, linear_key.T, forget_down_factor.T, small,
        shrunk, up,
    )
    kv, local, decayed, gate = call(
        local_kernel,
        (
            shape((2 * BLOCK, VDIM), BF16),
            shape((BLOCK, VDIM), F32),
            shape((BLOCK, HEAD), BF16),
            shape((BLOCK, VDIM), F32),
        ),
        scratch=[pltpu.VMEM((BLOCK, BLOCK), F32)],
        inputs=9,
    )(
        normed, differential_key, differential_value, linear_output_gate, linear_query.T, lk, lv,
        total, small,
    )
    team = exchanged(team, TEAM)
    far = call(group_kernel, shape((2 * BLOCK + 32, VDIM), BF16), inputs=2)(team, kv)
    far = lax.all_gather(far, "far")
    parts = call(
        attend_kernel,
        shape((MEMBERS, 2 * BLOCK + 16, VDIM), BF16),
        scratch=[
            pltpu.VMEM((MEMBERS * BLOCK, VDIM), BF16),
            pltpu.VMEM((GROUPS * BLOCK, VDIM), BF16),
            pltpu.VMEM((GROUPS * BLOCK, 2 * VDIM), BF16),
            pltpu.VMEM((BLOCK, VDIM), F32),
        ],
        scalars=1,
        inputs=3,
    )(place, second_map_weight.reshape(1, 1), team, far)
    parts = exchanged(parts, TEAM)
    mixed = call(finish_kernel, shape((BLOCK, differential_output_rows.shape[1]), BF16), inputs=7)(
        parts, local, decayed, gate, small, differential_output_rows, linear_output_rows
    )
    arrived = exchanged(mixed.reshape(copies, BLOCK // copies, -1), TP)
    return arrived.astype(F32).sum(axis=0).astype(BF16)


def solution(mesh):
    torus = Mesh(
        mesh.devices.reshape(GROUPS, 2, 4, mesh.shape["tp"] // 2, 2),
        ("far", "pair", "y", "x", "core"),
    )
    cols, lines = P(None, TP), P(TP, None)
    placed = (
        P(SP_TP, None), P(), cols, cols, cols, P(), P(), P(TP), P(), cols, cols, cols, cols,
        P(), cols, P(TP), P(SP, TP), P(), lines, lines,
    )
    return jax.shard_map(
        per_device, mesh=torus, in_specs=placed, out_specs=P(SP_TP, None), check_vma=False
    )
```

```python
import jax
import jax.numpy as jnp
from jax import lax
from jax.experimental import pallas as pl
from jax.experimental.pallas import tpu as pltpu
from jax.sharding import Mesh
from jax.sharding import PartitionSpec as P

F32 = jnp.float32
BF16 = jnp.bfloat16
HEAD = 64
VDIM = 128
BLOCK = 128
SUB = 16
GROUPS = 8
MEMBERS = 8
SP = ("far", "pair", "y")
TEAM = ("pair", "y")
TP = ("x", "core")
SP_TP = ("far", "pair", "y", "x", "core")
RMS_EPS = 1e-06
NEG_LARGE = -1e30
NT = (((1,), (1,)), ((), ()))


def two_parts(x):
    high = x.astype(BF16).astype(F32)
    return high, (x - high).astype(BF16).astype(F32)


def three_parts(x):
    high, rest = x.astype(BF16).astype(F32), None
    middle = (x - high).astype(BF16).astype(F32)
    rest = ((x - high) - middle).astype(BF16).astype(F32)
    return high, middle, rest


def dot(a, b):
    return jnp.dot(a, b, preferred_element_type=F32)


def dot_nt(a, b):
    return lax.dot_general(a, b, NT, preferred_element_type=F32)


def iota(shape, dim):
    return lax.broadcasted_iota(jnp.int32, shape, dim)


def two_map_norm(values, gain):
    first = iota(values.shape, 1) < HEAD
    squares = values * values
    low = jnp.sum(jnp.where(first, squares, 0.0), axis=1, keepdims=True)
    high = jnp.sum(jnp.where(first, 0.0, squares), axis=1, keepdims=True)
    mean_sq = jnp.where(first, low, high) * (1.0 / HEAD)
    return values * lax.rsqrt(mean_sq + RMS_EPS) * gain


def prepare_kernel(
    bias_ref, shrink_ref, qgain_ref, kgain_ref, dgain_ref, lgain_ref, gain_ref, up_ref,
    small_ref, shrunk_ref, ready_gain_ref, ready_up_ref,
):
    small_ref[0:1] = jnp.concatenate([qgain_ref[...]] * 2, axis=1)
    small_ref[1:2] = jnp.concatenate([kgain_ref[...]] * 2, axis=1)
    small_ref[2:3] = jnp.concatenate([bias_ref[...]] * 2, axis=1)
    small_ref[3:4] = dgain_ref[...]
    small_ref[4:5] = lgain_ref[...]
    small_ref[5:] = jnp.zeros((3, VDIM), F32)
    shrunk_ref[...] = jnp.broadcast_to(shrink_ref[...], shrunk_ref.shape).T
    ready_gain_ref[...] = gain_ref[...]
    ready_up_ref[...] = up_ref[...]


def copy_kernel(tokens_ref, copies_ref):
    tokens = tokens_ref[...]
    for chip in range(copies_ref.shape[0]):
        copies_ref[chip] = tokens


def project_kernel(
    rows_ref, gain_ref, dq_ref, lv_ref, lk_ref, down_ref, small_ref, shrunk_ref, up_ref,
    team_ref, normed_ref, lk_out_ref, lv_out_ref, total_ref,
):
    rows = jnp.concatenate(
        [rows_ref[core, chip] for chip in range(rows_ref.shape[1]) for core in range(2)], axis=0
    ).astype(F32)
    mean_sq = jnp.mean(rows * rows, axis=1, keepdims=True)
    normed = (rows * lax.rsqrt(mean_sq + RMS_EPS) * gain_ref[...]).astype(BF16)
    normed_ref[...] = normed

    narrow = dot_nt(normed, jnp.concatenate([lk_ref[...], down_ref[...]], axis=0)).astype(BF16)
    lk, low = narrow[:, :HEAD], narrow[:, HEAD:]
    lv = dot(normed, lv_ref[...]).astype(BF16)
    lk_out_ref[...] = lk
    lv_out_ref[...] = lv

    query = two_map_norm(dot(normed, dq_ref[...]).astype(BF16).astype(F32), small_ref[0:1])
    query = query.astype(BF16) * jnp.asarray(HEAD**-0.5, BF16)

    pre = dot(low, up_ref[...]) + small_ref[2:3, 0:HEAD]
    log_sig = jnp.minimum(pre, 0.0) - jnp.log1p(jnp.exp(-jnp.abs(pre)))
    log_a = log_sig * (1.0 / 16.0) + shrunk_ref[:, 0:HEAD]
    lower = (iota((BLOCK, BLOCK), 0) >= iota((BLOCK, BLOCK), 1)).astype(BF16)
    total = sum(dot(lower, piece.astype(BF16)) for piece in three_parts(log_a))

    total_ref[...] = total
    k_end = lk.astype(F32) * jnp.exp(total[BLOCK - 1 :] - total)
    flipped = jnp.concatenate([total, k_end], axis=1).T
    decay = jnp.broadcast_to(flipped[:HEAD, BLOCK - 1 :], (HEAD, VDIM))
    state = dot(flipped[HEAD:].astype(BF16), lv)
    state_parts = two_parts(state)
    decay_parts = two_parts(decay)
    for member in range(MEMBERS):
        own = slice(member * 8, member * 8 + 8)
        team_ref[member, 0:BLOCK] = query
        team_ref[member, BLOCK:] = jnp.concatenate(
            [piece[own] for piece in (*state_parts, *decay_parts)], axis=0
        ).astype(BF16)


def local_kernel(
    normed_ref, dk_ref, dv_ref, lg_ref, lq_ref, lk_ref, lv_ref, total_ref, small_ref,
    kv_ref, local_ref, decayed_ref, gate_ref, scores_ref,
):
    normed = normed_ref[...]
    key = two_map_norm(dot(normed, dk_ref[...]).astype(BF16).astype(F32), small_ref[1:2])
    kv_ref[0:BLOCK] = key.astype(BF16)
    kv_ref[BLOCK:] = dot(normed, dv_ref[...]).astype(BF16)
    gate = dot(normed, lg_ref[...]).astype(BF16).astype(F32)
    gate_ref[...] = gate * jax.nn.sigmoid(gate)
    lq = dot_nt(normed, lq_ref[...]).astype(BF16).astype(F32) * HEAD**-0.5
    lk = lk_ref[...].astype(F32)
    lv = lv_ref[...]
    total = total_ref[...]
    scores_ref[...] = jnp.zeros_like(scores_ref)
    for step in range(1, BLOCK // SUB):
        at = step * SUB
        border = total[at - 1 : at]
        q_part = lq[at : at + SUB] * jnp.exp(total[at : at + SUB] - border)
        k_part = lk[:at] * jnp.exp(border - total[:at])
        scores_ref[at : at + SUB, 0:at] = dot_nt(q_part.astype(BF16), k_part.astype(BF16))
    scores = scores_ref[...]
    row = iota((BLOCK, BLOCK), 0)
    distance = row - iota((BLOCK, BLOCK), 1)
    for shift in range(SUB):
        k_part = lk if shift == 0 else pltpu.roll(lk, shift, 0)
        if shift == 0:
            terms = lq * k_part
        else:
            terms = lq * k_part * jnp.exp(jnp.minimum(total - pltpu.roll(total, shift, 0), 0.0))
        column = jnp.sum(terms, axis=1, keepdims=True)
        here = (distance == shift) & (row % SUB >= shift)
        scores = jnp.where(here, column, scores)
    local_ref[...] = dot(scores.astype(BF16), lv)
    decayed_ref[...] = (lq * jnp.exp(total)).astype(BF16)


def joined(block, at):
    return block[at : at + 8] + block[at + 8 : at + 16]


def group_kernel(team_ref, kv_ref, out_ref):
    state = jnp.zeros((8, VDIM), F32)
    decay = jnp.zeros((8, VDIM), F32)
    for member in range(MEMBERS):
        block = team_ref[member, BLOCK:].astype(F32)
        own = joined(block, 16)
        state = state * jnp.exp(own) + joined(block, 0)
        decay = decay + own
    tail = jnp.concatenate([*two_parts(state), *two_parts(decay)], axis=0).astype(BF16)
    out_ref[0 : 2 * BLOCK] = kv_ref[...]
    out_ref[2 * BLOCK :] = tail


def attend_kernel(
    place_ref, weight_ref, team_ref, far_ref, out_ref, query_ref, key_ref, value_ref, logs_ref
):
    group, member = place_ref[0], place_ref[1]
    second_weight = weight_ref[0, 0]
    for other in range(GROUPS):
        span = slice(other * BLOCK, (other + 1) * BLOCK)
        query_ref[span] = team_ref[other, 0:BLOCK]
        key_ref[span] = far_ref[other, 0:BLOCK]
        value_ref[span, 0:VDIM] = far_ref[other, BLOCK : 2 * BLOCK]
    value_ref[:, VDIM:] = jnp.ones((GROUPS * BLOCK, VDIM), BF16)

    column = iota((1, 2 * BLOCK), 1)
    key_pos = (column // BLOCK * MEMBERS + member) * BLOCK + column % BLOCK
    lane = iota((BLOCK, VDIM), 1)
    logs_ref[...] = jnp.zeros_like(logs_ref)

    def attend(blocks):
        cols, open_cols = blocks * BLOCK, (blocks - 2) * BLOCK
        last_pos = key_pos + (blocks - 2) * MEMBERS * BLOCK
        batch = {2: 8, 4: 8, 6: 4}.get(blocks, 2)
        rows = batch * BLOCK

        def one(step, _):
            start = pl.multiple_of(step * rows, rows)
            causal = last_pos <= group * MEMBERS * BLOCK + start + iota((rows, 1), 0)
            found, logs = [], []
            for which in range(2):
                half = slice(which * HEAD, (which + 1) * HEAD)
                query = query_ref[pl.ds(start, rows), half]
                scores = dot_nt(query, key_ref[open_cols:cols, half])
                scores = jnp.where(causal, scores, NEG_LARGE)
                if open_cols:
                    scores = jnp.concatenate(
                        [dot_nt(query, key_ref[0:open_cols, half]), scores], axis=1
                    )
                peak = jnp.max(scores, axis=1, keepdims=True)
                weights = jnp.exp(scores - peak).astype(BF16)
                both = dot(weights, value_ref[0:cols])
                sums = both[:, VDIM:]
                found.append(both[:, :VDIM] / sums)
                logs.append(peak + jnp.log(sums))
            gap = found[0] - second_weight * found[1]
            total = logs_ref[...]
            for near in range(batch):
                index = step * batch + near
                part = slice(near * BLOCK, (near + 1) * BLOCK)
                out_ref[index, 0:BLOCK] = found[0][part].astype(BF16)
                out_ref[index, BLOCK : 2 * BLOCK] = gap[part].astype(BF16)
                for which in range(2):
                    total = jnp.where(lane == 2 * index + which, logs[which][part], total)
            logs_ref[...] = total
            return _

        if batch == MEMBERS:
            one(0, 0)
        else:
            lax.fori_loop(0, MEMBERS // batch, one, 0, unroll=True)

    for blocks in range(2, GROUPS + 1, 2):
        pl.when(group // 2 == blocks // 2 - 1)(lambda blocks=blocks: attend(blocks))
    logs = logs_ref[...]

    carried = jnp.zeros((8, VDIM), F32)
    for other in range(GROUPS):
        block = far_ref[other, 2 * BLOCK :].astype(F32)
        carried = jnp.where(
            other < group, carried * jnp.exp(joined(block, 16)) + joined(block, 0), carried
        )
    log_parts = three_parts(logs.T[: 2 * MEMBERS])
    for index in range(MEMBERS):
        pair = slice(2 * index, 2 * index + 2)
        tail = jnp.concatenate(
            [part[pair] for part in log_parts]
            + [jnp.zeros((10, VDIM), F32), *two_parts(carried)],
            axis=0,
        )
        out_ref[index, 2 * BLOCK :] = tail.astype(BF16)
        block = team_ref[index, BLOCK:].astype(F32)
        carried = carried * jnp.exp(joined(block, 16)) + joined(block, 0)


def finish_kernel(
    parts_ref, local_ref, decayed_ref, gate_ref, small_ref, drows_ref, lrows_ref, out_ref
):
    logs, states = [[], []], []
    for member in range(MEMBERS):
        tail = parts_ref[member, 2 * BLOCK :].astype(F32)
        for which in range(2):
            logs[which].append(
                tail[which : which + 1] + tail[which + 2 : which + 3] + tail[which + 4 : which + 5]
            )
        states.append(tail[16:24] + tail[24:32])
    shares = []
    for which in range(2):
        stacked = jnp.concatenate(logs[which], axis=0)
        raised = jnp.exp(stacked - jnp.max(stacked, axis=0, keepdims=True))
        shares.append(raised / jnp.sum(raised, axis=0, keepdims=True))
    factors = jnp.concatenate(
        [shares[0] - shares[1], shares[1], jnp.zeros((BLOCK - 2 * MEMBERS, VDIM), F32)], axis=0
    ).T
    mixed = jnp.zeros((BLOCK, VDIM), F32)
    for member in range(MEMBERS):
        first = parts_ref[member, 0:BLOCK].astype(F32)
        gap = parts_ref[member, BLOCK : 2 * BLOCK].astype(F32)
        mixed = mixed + factors[:, member : member + 1] * first
        mixed = mixed + factors[:, MEMBERS + member : MEMBERS + member + 1] * gap
    mean_sq = jnp.mean(mixed * mixed, axis=1, keepdims=True)
    attn = (0.8 * (mixed * lax.rsqrt(mean_sq + RMS_EPS) * small_ref[3:4])).astype(BF16)

    state = jnp.concatenate(states, axis=0).astype(BF16)
    chain = local_ref[...] + dot(decayed_ref[...], state)
    mean_sq = jnp.mean(chain * chain, axis=1, keepdims=True)
    chain = (chain * lax.rsqrt(mean_sq + RMS_EPS) * small_ref[4:5] * gate_ref[...]).astype(BF16)
    out_ref[...] = (dot(attn, drows_ref[...]) + dot(chain, lrows_ref[...])).astype(BF16)


def call(kernel, outs, scratch=(), scalars=0, inputs=0):
    vmem = pl.BlockSpec(memory_space=pltpu.VMEM)
    smem = pl.BlockSpec(memory_space=pltpu.SMEM)
    return pl.pallas_call(
        kernel,
        in_specs=[smem] * scalars + [vmem] * inputs,
        out_specs=jax.tree.map(lambda _: vmem, outs),
        out_shape=outs,
        scratch_shapes=scratch,
        compiler_params=pltpu.CompilerParams(vmem_limit_bytes=48 * 2**20),
    )


def exchanged(blocks, axis):
    return lax.all_to_all(blocks, axis, split_axis=0, concat_axis=0, tiled=True)


def per_device(
    tokens, input_norm_gain, differential_query, differential_key, differential_value,
    query_norm_gain, key_norm_gain, second_map_weight, differential_norm_gain, linear_query,
    linear_key, linear_value, linear_output_gate, forget_down_factor, forget_up_factor,
    forget_bias, extra_shrinkage_exponent, linear_norm_gain, differential_output_rows,
    linear_output_rows,
):
    shape = jax.ShapeDtypeStruct
    copies = lax.axis_size(TP)
    rows = call(copy_kernel, shape((copies // 2, *tokens.shape), BF16), inputs=1)(tokens)
    rows = exchanged(rows, "x")
    rows = lax.all_gather(rows, "core")
    place = jnp.stack([lax.axis_index("far"), lax.axis_index(TEAM)]).astype(jnp.int32)

    features = tokens.shape[1]
    small, shrunk, gain, up = call(
        prepare_kernel,
        (
            shape((8, VDIM), F32),
            shape((BLOCK, VDIM), F32),
            shape((1, features), F32),
            shape(forget_up_factor.shape, BF16),
        ),
        inputs=8,
    )(
        forget_bias.reshape(1, -1), extra_shrinkage_exponent.reshape(1, -1),
        query_norm_gain.reshape(1, -1), key_norm_gain.reshape(1, -1),
        differential_norm_gain.reshape(1, -1), linear_norm_gain.reshape(1, -1),
        input_norm_gain.reshape(1, -1), forget_up_factor,
    )
    team, normed, lk, lv, total = call(
        project_kernel,
        (
            shape((MEMBERS, BLOCK + 32, VDIM), BF16),
            shape((BLOCK, features), BF16),
            shape((BLOCK, HEAD), BF16),
            shape((BLOCK, VDIM), BF16),
            shape((BLOCK, HEAD), F32),
        ),
        inputs=9,
    )(
        rows, gain, differential_query, linear_value, linear_key.T, forget_down_factor.T, small,
        shrunk, up,
    )
    kv, local, decayed, gate = call(
        local_kernel,
        (
            shape((2 * BLOCK, VDIM), BF16),
            shape((BLOCK, VDIM), F32),
            shape((BLOCK, HEAD), BF16),
            shape((BLOCK, VDIM), F32),
        ),
        scratch=[pltpu.VMEM((BLOCK, BLOCK), F32)],
        inputs=9,
    )(
        normed, differential_key, differential_value, linear_output_gate, linear_query.T, lk, lv,
        total, small,
    )
    team = exchanged(team, TEAM)
    far = call(group_kernel, shape((2 * BLOCK + 32, VDIM), BF16), inputs=2)(team, kv)
    far = lax.all_gather(far, "far")
    parts = call(
        attend_kernel,
        shape((MEMBERS, 2 * BLOCK + 32, VDIM), BF16),
        scratch=[
            pltpu.VMEM((MEMBERS * BLOCK, VDIM), BF16),
            pltpu.VMEM((GROUPS * BLOCK, VDIM), BF16),
            pltpu.VMEM((GROUPS * BLOCK, 2 * VDIM), BF16),
            pltpu.VMEM((BLOCK, VDIM), F32),
        ],
        scalars=1,
        inputs=3,
    )(place, second_map_weight.reshape(1, 1), team, far)
    parts = exchanged(parts, TEAM)
    mixed = call(finish_kernel, shape((BLOCK, differential_output_rows.shape[1]), BF16), inputs=7)(
        parts, local, decayed, gate, small, differential_output_rows, linear_output_rows
    )
    arrived = exchanged(mixed.reshape(copies, BLOCK // copies, -1), TP)
    return arrived.astype(F32).sum(axis=0).astype(BF16)


def solution(mesh):
    torus = Mesh(
        mesh.devices.reshape(GROUPS, 2, 4, mesh.shape["tp"] // 2, 2),
        ("far", "pair", "y", "x", "core"),
    )
    cols, lines = P(None, TP), P(TP, None)
    placed = (
        P(SP_TP, None), P(), cols, cols, cols, P(), P(), P(TP), P(), cols, cols, cols, cols,
        P(), cols, P(TP), P(SP, TP), P(), lines, lines,
    )
    return jax.shard_map(
        per_device, mesh=torus, in_specs=placed, out_specs=P(SP_TP, None), check_vma=False
    )
```
